32 devices in a mesh: kv: 16 (over z, y, x), tp: 2 (over core).
Axes of the slice: x: 2, y: 2, z: 4, core: 2. Of those that a mesh axis runs over, the one named last changes fastest.
Arguments:
- tokens: bfloat16 [8, 2048, 2048], P(None, 'kv'), may hold values from -32 to 32, as said below
- w_query: bfloat16 [2048, 1024], P(None, 'tp'), may hold values from -0.125 to 0.125
- w_key: bfloat16 [2048, 512], P(None, 'tp'), may hold values from -0.125 to 0.125
- w_value: bfloat16 [2048, 512], P(None, 'tp'), may hold values from -0.125 to 0.125
- w_output: bfloat16 [1024, 2048], P(None, 'tp'), may hold values from -3 to 3
- chosen: int32 [8, 16, 32], P(None, 'kv'), may hold values from -1 to 15, as said below
- lengths: int32 [8], replicated, may hold values from 1 to 2048, 5632 in all
Outputs:
- mixed: bfloat16 [8, 2048, 2048], P(None, 'kv', 'tp')
The draws below stay inside these ranges and needn't reach their ends.
Inputs may be any that keep to these rules, and one draw needn't show every extreme that they name: chosen[s, b] lists distinct blocks of sequence s, none above b; its first entry is b; entries after the named ones are -1. For b >= 1 and each c < b, at most 4 of the 8 lists chosen[:, b] name block c, and exactly 4 of them name block b - 1. lengths[s] is the number of live positions of sequence s; the largest is 2048. `tokens`: activations of order one; some rows may be much larger.
All inputs are finite; a program needn't handle non-finite values.
Results may differ from the reference program's by a relative error of at most 0.012.
The reference program's roundings to bfloat16 on the way count: a program that leaves them out, or rounds other values in their place, can miss the bound.
Values may be sent and summed in bfloat16 or wider, within the bound.
No kernel may reach another device: no remote copies, remote signals or barrier semaphores. Data moves between devices by JAX's collectives and lax.ppermute only.
A program may use at most 128 MiB of HBM per device.

```python
import math
import jax
import jax.numpy as jnp
import numpy as np
from jax import lax

D = 2048
HEADS = 16
KV_HEADS = 8
HEAD_DIM = 64
BLK = 128
SEL = 32
SEQS = 8
CAP = 4
SEQ_LEN = 2048
BLOCKS_PER_SEQ = 16


def draw_tokens(key, part):
    shape = (SEQS, SEQ_LEN, D)
    return jnp.clip(jax.random.normal(key, shape, jnp.float32), -6.0, 6.0).astype(jnp.bfloat16)


def draw_chosen(key, part):
    key_allow, key_ordering = jax.random.split(jax.random.fold_in(key, 7))
    owners = jnp.arange(BLOCKS_PER_SEQ, dtype=jnp.int32)
    raw_scores = jax.random.randint(key_allow, (BLOCKS_PER_SEQ, BLOCKS_PER_SEQ, SEQS), 0, 1 << 20) * SEQS + jnp.arange(SEQS, dtype=jnp.int32)
    beaten = jnp.sum((raw_scores[:, :, None, :] > raw_scores[:, :, :, None]).astype(jnp.int32), axis=-1)
    permitted = beaten < CAP
    shard_member = owners[:, None]
    block_keeper = owners[None, :]
    earlier = block_keeper < shard_member
    candidate = earlier[None, :, :] & jnp.transpose(permitted, (2, 0, 1))
    own_block = (block_keeper == shard_member)[None, :, :]
    extra_score = jnp.where(block_keeper == shard_member, 4, jnp.where(block_keeper == shard_member - 1, 3, jnp.where(block_keeper == shard_member - BLOCKS_PER_SEQ // 2, 2, jnp.where(block_keeper == 0, 1, 0))))
    random_jitter = jax.random.randint(key_ordering, (SEQS, BLOCKS_PER_SEQ, BLOCKS_PER_SEQ), 0, 1 << 16)
    block_precedence = (extra_score[None, :, :] * (1 << 20) + random_jitter) * BLOCKS_PER_SEQ + block_keeper[None, :, :]
    block_precedence = jnp.where(candidate | own_block, block_precedence, -1)
    slot_count = min(SEL, BLOCKS_PER_SEQ)
    ranked, _ = lax.top_k(block_precedence, slot_count)
    picked = jnp.where(ranked >= 0, ranked % BLOCKS_PER_SEQ, -1)
    if slot_count < SEL:
        picked = jnp.concatenate([picked, jnp.full((SEQS, BLOCKS_PER_SEQ, SEL - slot_count), -1, jnp.int32)], axis=-1)
    return picked.astype(jnp.int32)


def block_scale(stream_key, dims, shards, smallest, largest):
    factor_of, own = 1.0, jax.random.fold_in(stream_key, 6)
    for axis_at, shards_of in shards:
        draws = jnp.exp(jax.random.uniform(jax.random.fold_in(own, axis_at), (shards_of,), jnp.float32, smallest / len(shards), largest / len(shards)))
        factor_of = factor_of * jnp.repeat(draws, dims[axis_at] // shards_of).reshape([-1 if axis == axis_at else 1 for axis in range(len(dims))])
    return factor_of


def split_up(number_of, total, reach, slope):
    loads = [(1 << 20) // math.isqrt(standing ** slope) + 1 for standing in range(2, number_of + 1)]
    surplus, given = total - reach - (number_of - 1), [1] * (number_of - 1)
    while surplus > 0:
        candidates = [i for i in range(number_of - 1) if given[i] < reach]
        pool, left = sum([loads[i] for i in candidates]), surplus
        for i in candidates:
            addition = min(reach - given[i], max(1, left * loads[i] // pool), surplus)
            given[i] = given[i] + addition
            surplus = surplus - addition
    return np.array([reach] + given)


def ragged(rng, amount, total, limit, skew):
    if amount == 2:
        one = jax.random.randint(rng, (), max(1, total - limit), min(limit, total - 1) + 1)
        return jnp.stack([one, total - one])
    sizes = jnp.asarray(split_up(amount, total, limit, skew), jnp.int32)
    couples = (amount - 1) // 2
    donor, receiver = sizes[1:1 + 2 * couples:2], sizes[2:2 + 2 * couples:2]
    margin = jnp.minimum(donor - 1, limit - receiver)
    shifted = jax.random.randint(jax.random.fold_in(rng, 1), (couples,), 0, 1 << 20) % (margin + 1)
    sizes = sizes.at[1:1 + 2 * couples:2].set(donor - shifted).at[2:2 + 2 * couples:2].set(receiver + shifted)
    return sizes[jax.random.permutation(jax.random.fold_in(rng, 2), amount)]


def bell_draw(key, extent, spread, reach, cuts=(), kind=jnp.bfloat16):
    gain = block_scale(key, extent, cuts, -0.22, 0.18) if cuts else 1.0
    drawn = jax.random.normal(key, extent, jnp.float32) * spread * gain
    return jnp.minimum(jnp.maximum(drawn, -reach), reach).astype(kind)


def setup_inputs(seed: int = 0) -> dict:
    arg_keys = jax.random.split(jax.random.key(seed), 8)
    return {
        "tokens": draw_tokens(jax.random.fold_in(arg_keys[7], 71), 0),
        "w_query": bell_draw(arg_keys[1], (D, HEADS * HEAD_DIM), D ** -0.5, 0.125, ((1, 2),)),
        "w_key": bell_draw(arg_keys[2], (D, KV_HEADS * HEAD_DIM), D ** -0.5, 0.125, ((1, 2),)),
        "w_value": bell_draw(arg_keys[3], (D, KV_HEADS * HEAD_DIM), D ** -0.5, 0.125, ((1, 2),)),
        "w_output": bell_draw(arg_keys[4], (HEADS * HEAD_DIM, D), 0.5, 3.0, ((1, 2),)),
        "chosen": draw_chosen(jax.random.fold_in(arg_keys[7], 71), 0),
        "lengths": ragged(arg_keys[6], SEQS, SEQ_LEN + (SEQS - 1) * SEQ_LEN // 4, SEQ_LEN, 2).astype(jnp.int32),
    }


def attend_block(query_rows, key_seq, value_seq, pick_row, first_pos, length):
    clipped = jnp.maximum(pick_row, 0)
    key_rows = key_seq[clipped].reshape(SEL * BLK, KV_HEADS, HEAD_DIM).astype(jnp.float32)
    value_rows = value_seq[clipped].reshape(SEL * BLK, KV_HEADS, HEAD_DIM).astype(jnp.float32)
    grouped = query_rows.reshape(BLK, KV_HEADS, HEADS // KV_HEADS, HEAD_DIM).astype(jnp.float32)
    scores = jnp.einsum("qkgd,nkd->kgqn", grouped, key_rows) * HEAD_DIM ** -0.5
    query_pos = first_pos + jnp.arange(BLK, dtype=jnp.int32)
    key_pos = (pick_row[:, None] * BLK + jnp.arange(BLK, dtype=jnp.int32)[None, :]).reshape(-1)
    listed = jnp.repeat(pick_row >= 0, BLK)
    allowed = listed[None, :] & (key_pos[None, :] <= query_pos[:, None]) & (key_pos[None, :] < length)
    masked = jnp.where(allowed, scores, -1e30)
    row_max = jnp.max(masked, axis=-1, keepdims=True)
    exponent = jnp.exp(masked - row_max)
    weights = (exponent / jnp.sum(exponent, axis=-1, keepdims=True)).astype(jnp.bfloat16)
    weights = lax.optimization_barrier(weights).astype(jnp.float32)
    mixed_heads = jnp.einsum("kgqn,nkd->qkgd", weights, value_rows)
    live_rows = (query_pos < length)[:, None, None, None]
    return jnp.where(live_rows, mixed_heads, 0.0).astype(jnp.bfloat16).reshape(BLK, HEADS * HEAD_DIM)


def reference(tokens, w_query, w_key, w_value, w_output, chosen, lengths):
    flat_rows = tokens.reshape(SEQS * SEQ_LEN, D)
    queries = lax.optimization_barrier(jnp.dot(flat_rows, w_query, preferred_element_type=jnp.float32).astype(jnp.bfloat16))
    key_proj = lax.optimization_barrier(jnp.dot(flat_rows, w_key, preferred_element_type=jnp.float32).astype(jnp.bfloat16))
    value_proj = lax.optimization_barrier(jnp.dot(flat_rows, w_value, preferred_element_type=jnp.float32).astype(jnp.bfloat16))
    queries = queries.reshape(SEQS, BLOCKS_PER_SEQ, BLK, HEADS * HEAD_DIM)
    key_proj = key_proj.reshape(SEQS, BLOCKS_PER_SEQ, BLK, KV_HEADS, HEAD_DIM)
    value_proj = value_proj.reshape(SEQS, BLOCKS_PER_SEQ, BLK, KV_HEADS, HEAD_DIM)

    def one_seq(packed):
        query_seq, key_seq, value_seq, pick_seq, length = packed

        def one_block(inner_pack):
            query_rows, pick_row, block_id = inner_pack
            return attend_block(query_rows, key_seq, value_seq, pick_row, block_id * BLK, length)

        return lax.map(one_block, (query_seq, pick_seq, jnp.arange(BLOCKS_PER_SEQ, dtype=jnp.int32)))

    attended = lax.map(one_seq, (queries, key_proj, value_proj, chosen, lengths))
    mixed = jnp.dot(attended.reshape(SEQS * SEQ_LEN, HEADS * HEAD_DIM), w_output, preferred_element_type=jnp.float32)
    return mixed.astype(jnp.bfloat16).reshape(SEQS, SEQ_LEN, D)
```

```python
import functools

import jax
import jax.numpy as jnp
from jax import lax
from jax.experimental import pallas as pl
from jax.experimental.pallas import tpu as pltpu
from jax.sharding import PartitionSpec as P

HEADS = 16
KV_HEADS = 8
HEAD_DIM = 64
CAP = 4
META_ROWS = 16
LANES = 128
GROUP = 4


def per_device_general(tokens, w_query, w_key, w_value, w_output, chosen, lengths):
    seq_count, block_len, model_width = tokens.shape
    flat_rows = tokens.reshape(seq_count * block_len, model_width)
    queries = jnp.dot(flat_rows, w_query, preferred_element_type=jnp.float32).astype(jnp.bfloat16)
    key_proj = jnp.dot(flat_rows, w_key, preferred_element_type=jnp.float32).astype(jnp.bfloat16)
    value_proj = jnp.dot(flat_rows, w_value, preferred_element_type=jnp.float32).astype(
        jnp.bfloat16
    )
    key_width = key_proj.shape[1]
    local_blocks = jnp.concatenate([key_proj, value_proj], axis=1).reshape(
        seq_count, block_len, 2 * key_width
    )
    shard_member = lax.axis_index("kv")
    kv_devices = lax.axis_size("kv")
    picked = chosen[:, 0, :]
    clipped = jnp.maximum(picked, 0)
    seq_index = jnp.arange(seq_count, dtype=jnp.int32)
    owners = jnp.arange(kv_devices, dtype=jnp.int32)
    wanted = (
        jnp.any(picked[:, :, None] == owners[None, None, :], axis=1)
        & (owners != shard_member)[None, :]
    )
    wanted = wanted.T
    ranked = jnp.cumsum(wanted.astype(jnp.int32), axis=1) - 1
    slot_hit = wanted[:, :, None] & (
        ranked[:, :, None] == jnp.arange(CAP, dtype=jnp.int32)[None, None, :]
    )
    request = jnp.sum(slot_hit.astype(jnp.int32) * (seq_index + 1)[None, :, None], axis=1) - 1
    incoming = lax.all_to_all(request, "kv", split_axis=0, concat_axis=0, tiled=True)
    outgoing = local_blocks[jnp.maximum(incoming, 0)]
    arrived = lax.all_to_all(outgoing, "kv", split_axis=0, concat_axis=0, tiled=True)
    key_lookup = jnp.concatenate(
        [local_blocks, arrived.reshape(kv_devices * CAP, block_len, 2 * key_width)], axis=0
    )
    rank_at = jnp.take_along_axis(ranked.T, clipped, axis=1)
    source = jnp.where(
        picked == shard_member, seq_index[:, None], seq_count + clipped * CAP + rank_at
    )
    group_size = HEADS // KV_HEADS
    local_kv_heads = key_width // HEAD_DIM
    query_pos = shard_member * block_len + jnp.arange(block_len, dtype=jnp.int32)
    score_scale = HEAD_DIM ** (-0.5)

    def attend(packed):
        query_rows, source_row, pick_row, length = packed
        fetched = key_lookup[source_row]
        slot_count = pick_row.shape[0]
        key_rows = fetched[:, :, :key_width].reshape(
            slot_count * block_len, local_kv_heads, HEAD_DIM
        )
        value_rows = fetched[:, :, key_width:].reshape(
            slot_count * block_len, local_kv_heads, HEAD_DIM
        )
        grouped = query_rows.reshape(block_len, local_kv_heads, group_size, HEAD_DIM)
        scores = (
            jnp.einsum("qkgd,nkd->kgqn", grouped, key_rows, preferred_element_type=jnp.float32)
            * score_scale
        )
        key_pos = (
            pick_row[:, None] * block_len + jnp.arange(block_len, dtype=jnp.int32)[None, :]
        ).reshape(-1)
        listed = jnp.repeat(pick_row >= 0, block_len)
        allowed = (
            listed[None, :] & (key_pos[None, :] <= query_pos[:, None]) & (key_pos[None, :] < length)
        )
        masked = jnp.where(allowed, scores, -1e30)
        row_max = jnp.max(masked, axis=-1, keepdims=True)
        exponent = jnp.exp(masked - row_max)
        weights = (exponent / jnp.sum(exponent, axis=-1, keepdims=True)).astype(jnp.bfloat16)
        mixed_heads = jnp.einsum(
            "kgqn,nkd->qkgd", weights, value_rows, preferred_element_type=jnp.float32
        )
        live_rows = (query_pos < length)[:, None, None, None]
        return jnp.where(live_rows, mixed_heads, 0.0).astype(jnp.bfloat16).reshape(block_len, -1)

    attended = lax.map(attend, (queries.reshape(seq_count, block_len, -1), source, picked, lengths))
    attended_rows = attended.reshape(seq_count * block_len, -1)
    summed = jnp.dot(
        lax.all_gather(attended_rows, "tp", axis=1, tiled=True),
        w_output,
        preferred_element_type=jnp.float32,
    )
    return summed.astype(jnp.bfloat16).reshape(seq_count, block_len, -1)


def project_kernel(order_ref, *refs, slots, kv_local):
    token_refs = refs[:slots]
    wq_ref, wk_ref, wv_ref, meta_ref, out_ref = refs[slots:]
    plane = pl.program_id(0)
    blk = token_refs[0].shape[1]
    rows = jnp.concatenate([t[0] for t in token_refs], axis=0)
    q = jnp.dot(rows, wq_ref[...], preferred_element_type=jnp.float32).astype(jnp.bfloat16)
    k = jnp.dot(rows, wk_ref[...], preferred_element_type=jnp.float32).astype(jnp.bfloat16)
    v = jnp.dot(rows, wv_ref[...], preferred_element_type=jnp.float32).astype(jnp.bfloat16)
    for h in range(kv_local):
        dest = plane * kv_local + h
        q_h = q[:, h * LANES:(h + 1) * LANES]
        kv_h = jnp.concatenate(
            [k[:, h * HEAD_DIM:(h + 1) * HEAD_DIM], v[:, h * HEAD_DIM:(h + 1) * HEAD_DIM]], axis=1
        )
        for j in range(slots):
            base = j * 2 * blk
            out_ref[dest, base:base + blk, :] = q_h[j * blk:(j + 1) * blk]
            out_ref[dest, base + blk:base + 2 * blk, :] = kv_h[j * blk:(j + 1) * blk]
        out_ref[dest, slots * 2 * blk:, :] = meta_ref[0]


def project(tokens, w_query, w_key, w_value, meta, order, planes, slots, kv_local):
    seq_count, blk, width = tokens.shape
    rows = slots * 2 * blk + META_ROWS

    def token_map(j):
        return lambda p, order_ref: (order_ref[j * planes + p], 0, 0)

    whole = lambda a: pl.BlockSpec(a.shape, lambda p, o: (0,) * a.ndim)
    dests = planes * kv_local
    return pl.pallas_call(
        functools.partial(project_kernel, slots=slots, kv_local=kv_local),
        grid_spec=pltpu.PrefetchScalarGridSpec(
            num_scalar_prefetch=1,
            grid=(planes,),
            in_specs=[pl.BlockSpec((1, blk, width), token_map(j)) for j in range(slots)]
            + [whole(w_query), whole(w_key), whole(w_value)]
            + [pl.BlockSpec((1, META_ROWS, LANES), lambda p, o: (p, 0, 0))],
            out_specs=pl.BlockSpec((dests, rows, LANES), lambda p, o: (0, 0, 0)),
        ),
        out_shape=jax.ShapeDtypeStruct((dests, rows, LANES), jnp.bfloat16),
        compiler_params=pltpu.CompilerParams(vmem_limit_bytes=48 << 20),
        cost_estimate=pl.CostEstimate(
            flops=2 * seq_count * blk * width * 2 * kv_local * LANES,
            transcendentals=0,
            bytes_accessed=2 * (tokens.size + w_query.size * 2 + dests * rows * LANES),
        ),
        name="project",
    )(order, *([tokens] * slots), w_query, w_key, w_value, meta)


def attend_kernel(lens_ref, list_ref, in_ref, out_ref, *, slots, blocks, blk, stride):
    lane = lax.broadcasted_iota(jnp.int32, (blk, LANES), 1)
    low = lane < HEAD_DIM
    scale = HEAD_DIM ** -0.5

    def one(j, b, length):
        base = pl.multiple_of(j * 2 * blk, 2 * blk)
        meta = (b * slots + j) * LANES
        q = in_ref[b, pl.ds(base, blk), :]
        rolled = jnp.where(low, pltpu.roll(q.astype(jnp.float32), HEAD_DIM, 1), 0.0)
        q0 = jnp.where(low, q.astype(jnp.float32), 0.0)
        q2 = (jnp.concatenate([q0, rolled], axis=0) * scale).astype(jnp.bfloat16)
        count = list_ref[meta + stride]

        def body(groups):
            total = groups * GROUP
            kvs = []
            for t in range(total):
                c = jnp.maximum(list_ref[meta + t], 0)
                kvs.append(in_ref[c, pl.ds(base + blk, blk), :])
            kv = jnp.concatenate(kvs, axis=0)
            s = lax.dot_general(
                q2, kv, (((1,), (1,)), ((), ())), preferred_element_type=jnp.float32
            )
            row = lax.broadcasted_iota(jnp.int32, (2 * blk, blk), 0) % blk
            col = lax.broadcasted_iota(jnp.int32, (2 * blk, blk), 1)
            parts = []
            for t in range(total):
                part = s[:, t * blk:(t + 1) * blk]
                if t == 0:
                    part = jnp.where(col <= row, part, -1e30)
                elif t > total - GROUP:
                    part = jnp.where(t < count, part, -1e30)
                parts.append(part)
            peak = parts[0]
            for part in parts[1:]:
                peak = jnp.maximum(peak, part)
            m = jnp.max(peak, axis=1, keepdims=True)
            exps = [jnp.exp(part - m) for part in parts]
            acc = exps[0]
            for e in exps[1:]:
                acc = acc + e
            denom = jnp.sum(acc, axis=1, keepdims=True)
            p = jnp.concatenate([e.astype(jnp.bfloat16) for e in exps], axis=1)
            o = jnp.dot(p, kv, preferred_element_type=jnp.float32) / denom
            o = jnp.where(low, pltpu.roll(o[:blk], HEAD_DIM, 1), o[blk:])
            pos = b * blk + lax.broadcasted_iota(jnp.int32, (blk, LANES), 0)
            out_ref[b, pl.ds(pl.multiple_of(j * blk, blk), blk), :] = jnp.where(
                pos < length, o, 0.0
            ).astype(jnp.bfloat16)

        for groups in range(1, -(-blocks // GROUP) + 1):
            @pl.when((count > (groups - 1) * GROUP) & (count <= groups * GROUP))
            def _():
                body(groups)

    for j in range(slots):
        length = lens_ref[j]

        @pl.loop(0, blocks)
        def _(b):
            @pl.when(b * blk < length)
            def _():
                one(j, b, length)

            @pl.when(b * blk >= length)
            def _():
                out_ref[b, j * blk:(j + 1) * blk, :] = jnp.zeros((blk, LANES), jnp.bfloat16)


def attend(arrived, lens, lists, slots, blk, stride):
    blocks = arrived.shape[0]
    return pl.pallas_call(
        functools.partial(attend_kernel, slots=slots, blocks=blocks, blk=blk, stride=stride),
        grid_spec=pltpu.PrefetchScalarGridSpec(
            num_scalar_prefetch=2,
            grid=(1,),
            in_specs=[pl.BlockSpec(arrived.shape, lambda i, a, b: (0, 0, 0))],
            out_specs=pl.BlockSpec((blocks, slots * blk, LANES), lambda i, a, b: (0, 0, 0)),
        ),
        out_shape=jax.ShapeDtypeStruct((blocks, slots * blk, LANES), jnp.bfloat16),
        compiler_params=pltpu.CompilerParams(vmem_limit_bytes=48 << 20),
        cost_estimate=pl.CostEstimate(
            flops=4 * 2 * blk * blk * LANES * 100, transcendentals=0, bytes_accessed=3 << 20
        ),
        name="attend",
    )(lens, lists, arrived)


def output_kernel(order_ref, own_ref, other_ref, w_ref, out_ref, *, slots, planes, kv_local):
    plane = pl.program_id(0)
    blk = out_ref.shape[1]
    half = kv_local * LANES
    side = order_ref[slots * planes]

    def rows(ref):
        return jnp.concatenate(
            [
                jnp.concatenate([ref[h, j * blk:(j + 1) * blk, :] for h in range(kv_local)], axis=1)
                for j in range(slots)
            ],
            axis=0,
        )

    own_at = pl.multiple_of(side * half, half)
    other_at = pl.multiple_of((1 - side) * half, half)
    o = jnp.dot(rows(own_ref), w_ref[pl.ds(own_at, half), :], preferred_element_type=jnp.float32)
    o = o + jnp.dot(
        rows(other_ref), w_ref[pl.ds(other_at, half), :], preferred_element_type=jnp.float32
    )
    o = o.astype(jnp.bfloat16)
    for j in range(slots):
        out_ref[order_ref[j * planes + plane]] = o[j * blk:(j + 1) * blk]


def output_projection(own, other, w_output, order, planes, slots, kv_local, blk):
    seq_count = planes * slots
    width = w_output.shape[1]
    return pl.pallas_call(
        functools.partial(output_kernel, slots=slots, planes=planes, kv_local=kv_local),
        grid_spec=pltpu.PrefetchScalarGridSpec(
            num_scalar_prefetch=1,
            grid=(planes,),
            in_specs=[
                pl.BlockSpec((kv_local, slots * blk, LANES), lambda p, o: (p, 0, 0)),
                pl.BlockSpec((kv_local, slots * blk, LANES), lambda p, o: (p, 0, 0)),
                pl.BlockSpec(w_output.shape, lambda p, o: (0, 0)),
            ],
            out_specs=pl.BlockSpec((seq_count, blk, width), lambda p, o: (0, 0, 0)),
        ),
        out_shape=jax.ShapeDtypeStruct((seq_count, blk, width), jnp.bfloat16),
        compiler_params=pltpu.CompilerParams(vmem_limit_bytes=48 << 20),
        cost_estimate=pl.CostEstimate(
            flops=2 * seq_count * blk * w_output.size, transcendentals=0, bytes_accessed=6 << 20
        ),
        name="output_projection",
    )(order, own, other, w_output)


def per_device(tokens, w_query, w_key, w_value, w_output, chosen, lengths):
    seq_count, blk, _ = tokens.shape
    kv_devices = lax.axis_size("kv")
    kv_local = w_key.shape[1] // HEAD_DIM
    planes = kv_devices // kv_local
    slots = seq_count // planes
    select = chosen.shape[2]
    seq_ids = jnp.arange(seq_count, dtype=jnp.int32)
    longer = (lengths[None, :] > lengths[:, None]) | (
        (lengths[None, :] == lengths[:, None]) & (seq_ids[None, :] < seq_ids[:, None])
    )
    rank = jnp.sum(longer.astype(jnp.int32), axis=1)
    turn, step = rank // planes, rank % planes
    place = turn * planes + jnp.where(turn % 2 == 0, step, planes - 1 - step)
    order = jnp.sum(jnp.where(place[None, :] == seq_ids[:, None], seq_ids[None, :], 0), axis=1)

    picked = chosen[:, 0, :]
    count = jnp.sum((picked >= 0).astype(jnp.int32), axis=1, keepdims=True)
    meta = jnp.concatenate([picked, count], axis=1).astype(jnp.bfloat16)
    meta = jnp.pad(meta, ((0, 0), (0, LANES - select - 1)))
    hit = (order[:, None] == seq_ids[None, :]).astype(jnp.bfloat16)
    meta = jnp.dot(hit, meta, preferred_element_type=jnp.float32).astype(jnp.bfloat16)
    meta = meta.reshape(slots, planes, LANES).transpose(1, 0, 2)
    meta = jnp.pad(meta, ((0, 0), (0, META_ROWS - slots), (0, 0)))

    payload = project(
        tokens, w_query, w_key, w_value, meta, order, planes, slots, kv_local
    )
    arrived = lax.all_to_all(payload, "kv", split_axis=0, concat_axis=0, tiled=True)
    lists = arrived[:, slots * 2 * blk:slots * 2 * blk + slots, :].astype(jnp.int32).reshape(-1)
    my_plane = lax.axis_index("kv") // kv_local
    mine = jnp.arange(slots, dtype=jnp.int32) * planes + my_plane
    my_seqs = jnp.sum(jnp.where(mine[:, None] == seq_ids[None, :], order[None, :], 0), axis=1)
    lens = jnp.sum(jnp.where(my_seqs[:, None] == seq_ids[None, :], lengths[None, :], 0), axis=1)
    attended = attend(arrived, lens, lists, slots, blk, select)
    own = lax.all_to_all(attended, "kv", split_axis=0, concat_axis=0, tiled=True)
    other = lax.ppermute(own, "tp", [(0, 1), (1, 0)])
    order_side = jnp.concatenate([order, lax.axis_index("tp").astype(jnp.int32)[None]])
    return output_projection(own, other, w_output, order_side, planes, slots, kv_local, blk)


def fits(mesh, tokens, w_key, chosen):
    kv_devices, tp_devices = mesh.shape["kv"], mesh.shape["tp"]
    kv_local = w_key.shape[1] // tp_devices // HEAD_DIM
    if HEADS // KV_HEADS * HEAD_DIM != LANES or 2 * HEAD_DIM != LANES or tp_devices != 2:
        return False
    if kv_local == 0 or kv_devices % kv_local or kv_devices > 16 or chosen.shape[2] >= LANES:
        return False
    planes = kv_devices // kv_local
    blk = tokens.shape[1] // kv_devices
    return tokens.shape[0] % planes == 0 and tokens.shape[0] // planes <= META_ROWS and blk == LANES


def solution(mesh):
    def run(tokens, w_query, w_key, w_value, w_output, chosen, lengths):
        body = per_device if fits(mesh, tokens, w_key, chosen) else per_device_general
        return jax.shard_map(
            body,
            mesh=mesh,
            in_specs=(
                P(None, "kv", None),
                P(None, "tp"),
                P(None, "tp"),
                P(None, "tp"),
                P(None, "tp"),
                P(None, "kv", None),
                P(),
            ),
            out_specs=P(None, "kv", "tp"),
            check_vma=False,
        )(tokens, w_query, w_key, w_value, w_output, chosen, lengths)

    return run
```

```python
import functools

import jax
import jax.numpy as jnp
from jax import lax
from jax.experimental import pallas as pl
from jax.experimental.pallas import tpu as pltpu
from jax.sharding import PartitionSpec as P

HEADS = 16
KV_HEADS = 8
HEAD_DIM = 64
CAP = 4
META_ROWS = 16
LANES = 128
GROUP = 4
VMEM_MOST = 63 << 20
HBM = pltpu.HBM


def per_device_general(tokens, w_query, w_key, w_value, w_output, chosen, lengths):
    seq_count, block_len, model_width = tokens.shape
    flat_rows = tokens.reshape(seq_count * block_len, model_width)
    queries = jnp.dot(flat_rows, w_query, preferred_element_type=jnp.float32).astype(jnp.bfloat16)
    key_proj = jnp.dot(flat_rows, w_key, preferred_element_type=jnp.float32).astype(jnp.bfloat16)
    value_proj = jnp.dot(flat_rows, w_value, preferred_element_type=jnp.float32).astype(
        jnp.bfloat16
    )
    key_width = key_proj.shape[1]
    local_blocks = jnp.concatenate([key_proj, value_proj], axis=1).reshape(
        seq_count, block_len, 2 * key_width
    )
    shard_member = lax.axis_index("kv")
    kv_devices = lax.axis_size("kv")
    picked = chosen[:, 0, :]
    clipped = jnp.maximum(picked, 0)
    seq_index = jnp.arange(seq_count, dtype=jnp.int32)
    owners = jnp.arange(kv_devices, dtype=jnp.int32)
    wanted = (
        jnp.any(picked[:, :, None] == owners[None, None, :], axis=1)
        & (owners != shard_member)[None, :]
    )
    wanted = wanted.T
    ranked = jnp.cumsum(wanted.astype(jnp.int32), axis=1) - 1
    slot_hit = wanted[:, :, None] & (
        ranked[:, :, None] == jnp.arange(CAP, dtype=jnp.int32)[None, None, :]
    )
    request = jnp.sum(slot_hit.astype(jnp.int32) * (seq_index + 1)[None, :, None], axis=1) - 1
    incoming = lax.all_to_all(request, "kv", split_axis=0, concat_axis=0, tiled=True)
    outgoing = local_blocks[jnp.maximum(incoming, 0)]
    arrived = lax.all_to_all(outgoing, "kv", split_axis=0, concat_axis=0, tiled=True)
    key_lookup = jnp.concatenate(
        [local_blocks, arrived.reshape(kv_devices * CAP, block_len, 2 * key_width)], axis=0
    )
    rank_at = jnp.take_along_axis(ranked.T, clipped, axis=1)
    source = jnp.where(
        picked == shard_member, seq_index[:, None], seq_count + clipped * CAP + rank_at
    )
    group_size = HEADS // KV_HEADS
    local_kv_heads = key_width // HEAD_DIM
    query_pos = shard_member * block_len + jnp.arange(block_len, dtype=jnp.int32)
    score_scale = HEAD_DIM ** (-0.5)

    def attend(packed):
        query_rows, source_row, pick_row, length = packed
        fetched = key_lookup[source_row]
        slot_count = pick_row.shape[0]
        key_rows = fetched[:, :, :key_width].reshape(
            slot_count * block_len, local_kv_heads, HEAD_DIM
        )
        value_rows = fetched[:, :, key_width:].reshape(
            slot_count * block_len, local_kv_heads, HEAD_DIM
        )
        grouped = query_rows.reshape(block_len, local_kv_heads, group_size, HEAD_DIM)
        scores = (
            jnp.einsum("qkgd,nkd->kgqn", grouped, key_rows, preferred_element_type=jnp.float32)
            * score_scale
        )
        key_pos = (
            pick_row[:, None] * block_len + jnp.arange(block_len, dtype=jnp.int32)[None, :]
        ).reshape(-1)
        listed = jnp.repeat(pick_row >= 0, block_len)
        allowed = (
            listed[None, :] & (key_pos[None, :] <= query_pos[:, None]) & (key_pos[None, :] < length)
        )
        masked = jnp.where(allowed, scores, -1e30)
        row_max = jnp.max(masked, axis=-1, keepdims=True)
        exponent = jnp.exp(masked - row_max)
        weights = (exponent / jnp.sum(exponent, axis=-1, keepdims=True)).astype(jnp.bfloat16)
        mixed_heads = jnp.einsum(
            "kgqn,nkd->qkgd", weights, value_rows, preferred_element_type=jnp.float32
        )
        live_rows = (query_pos < length)[:, None, None, None]
        return jnp.where(live_rows, mixed_heads, 0.0).astype(jnp.bfloat16).reshape(block_len, -1)

    attended = lax.map(attend, (queries.reshape(seq_count, block_len, -1), source, picked, lengths))
    attended_rows = attended.reshape(seq_count * block_len, -1)
    summed = jnp.dot(
        lax.all_gather(attended_rows, "tp", axis=1, tiled=True),
        w_output,
        preferred_element_type=jnp.float32,
    )
    return summed.astype(jnp.bfloat16).reshape(seq_count, block_len, -1)


def order_by_length(lengths_ref, order_ref, seq_count):
    for s in range(seq_count):
        rank = jnp.int32(0)
        for t in range(seq_count):
            if t < s:
                ahead = lengths_ref[t] >= lengths_ref[s]
            elif t > s:
                ahead = lengths_ref[t] > lengths_ref[s]
            else:
                continue
            rank = rank + jnp.where(ahead, 1, 0)
        order_ref[rank] = s


def project_kernel(
    lengths_ref, chosen_ref, tokens_ref, wq_ref, wk_ref, wv_ref, out_ref,
    order_ref, meta_ref, rows_ref, wq_buf, wk_buf, wv_buf, row_sems, w_sems,
    *, ranks, slots, kv_local, select,
):
    seq_count = chosen_ref.shape[0]
    blk = tokens_ref.shape[1]
    loads = [
        pltpu.make_async_copy(wq_ref, wq_buf, w_sems.at[0]),
        pltpu.make_async_copy(wk_ref, wk_buf, w_sems.at[1]),
        pltpu.make_async_copy(wv_ref, wv_buf, w_sems.at[2]),
    ]
    order_by_length(lengths_ref, order_ref, seq_count)
    fetch = [
        pltpu.make_async_copy(
            tokens_ref.at[order_ref[rank]], rows_ref.at[pl.ds(i * blk, blk)], row_sems.at[i]
        )
        for i, rank in enumerate(ranks)
    ]
    for f in fetch[:2]:
        f.start()
    for load in loads:
        load.start()
    for f in fetch[2:]:
        f.start()
    meta_ref[...] = jnp.zeros(meta_ref.shape, jnp.float32)
    for s in range(seq_count):
        meta_ref[s:s + 1, :select] = chosen_ref[s].astype(jnp.float32)
    lane = lax.broadcasted_iota(jnp.int32, meta_ref.shape, 1)
    named = meta_ref[...]
    count = jnp.sum(jnp.where((lane < select) & (named >= 0), 1.0, 0.0), axis=1, keepdims=True)
    meta_ref[...] = jnp.where(lane == select, count, named)
    tile_row = lax.broadcasted_iota(jnp.int32, (META_ROWS, LANES), 0)
    planes = len(ranks) // slots
    for p in range(planes):
        tile = jnp.zeros((META_ROWS, LANES), jnp.float32)
        for j in range(slots):
            row = meta_ref[pl.ds(order_ref[ranks[p * slots + j]], 1), :]
            tile = jnp.where(tile_row == j, row, tile)
        tile = tile.astype(jnp.bfloat16)
        for h in range(kv_local):
            out_ref[p * kv_local + h, slots * 2 * blk:, :] = tile
    for load in loads:
        load.wait()
    for first in range(0, len(ranks), 2):
        fetch[first].wait()
        fetch[first + 1].wait()
        rows = rows_ref[first * blk:(first + 2) * blk, :]
        q = jnp.dot(rows, wq_buf[...], preferred_element_type=jnp.float32).astype(jnp.bfloat16)
        k = jnp.dot(rows, wk_buf[...], preferred_element_type=jnp.float32).astype(jnp.bfloat16)
        v = jnp.dot(rows, wv_buf[...], preferred_element_type=jnp.float32).astype(jnp.bfloat16)
        for h in range(kv_local):
            q_h = q[:, h * LANES:(h + 1) * LANES]
            kv_h = jnp.concatenate(
                [k[:, h * HEAD_DIM:(h + 1) * HEAD_DIM], v[:, h * HEAD_DIM:(h + 1) * HEAD_DIM]],
                axis=1,
            )
            for i in range(2):
                p, j = divmod(first + i, slots)
                base = j * 2 * blk
                out_ref[p * kv_local + h, base:base + blk, :] = q_h[i * blk:(i + 1) * blk]
                out_ref[p * kv_local + h, base + blk:base + 2 * blk, :] = kv_h[i * blk:(i + 1) * blk]


def project(tokens, w_query, w_key, w_value, chosen, lengths, ranks, slots, kv_local):
    seq_count, blk, width = tokens.shape
    dests = len(ranks) // slots * kv_local
    rows = slots * 2 * blk + META_ROWS
    hbm = pl.BlockSpec(memory_space=HBM)
    return pl.pallas_call(
        functools.partial(
            project_kernel, ranks=ranks, slots=slots, kv_local=kv_local, select=chosen.shape[2]
        ),
        in_specs=[
            pl.BlockSpec(memory_space=pltpu.SMEM),
            pl.BlockSpec(memory_space=pltpu.VMEM),
            hbm, hbm, hbm, hbm,
        ],
        out_specs=pl.BlockSpec(memory_space=pltpu.VMEM),
        out_shape=jax.ShapeDtypeStruct((dests, rows, LANES), jnp.bfloat16),
        scratch_shapes=[
            pltpu.SMEM((seq_count,), jnp.int32),
            pltpu.VMEM((seq_count, LANES), jnp.float32),
            pltpu.VMEM((len(ranks) * blk, width), jnp.bfloat16),
            pltpu.VMEM(w_query.shape, jnp.bfloat16),
            pltpu.VMEM(w_key.shape, jnp.bfloat16),
            pltpu.VMEM(w_value.shape, jnp.bfloat16),
            pltpu.SemaphoreType.DMA((len(ranks),)),
            pltpu.SemaphoreType.DMA((3,)),
        ],
        compiler_params=pltpu.CompilerParams(vmem_limit_bytes=VMEM_MOST),
        cost_estimate=pl.CostEstimate(
            flops=2 * len(ranks) * blk * width * 2 * kv_local * LANES,
            transcendentals=0,
            bytes_accessed=2 * (len(ranks) * blk * width + w_query.size * 2 + dests * rows * LANES),
        ),
        name="project",
    )(lengths, chosen, tokens, w_query, w_key, w_value)


def attend_kernel(
    lengths_ref, where_ref, list_ref, far_ref, *refs, slots, split, planes, blocks, blk, stride,
):
    parts = slots // split
    arrived, near, (out_ref, order_ref, q_buf, kv_buf, sems) = refs[:parts], refs[parts:-5], refs[-5:]
    plane, start = where_ref[0], where_ref[1]
    copies = []
    for j in range(slots):
        part, base = arrived[j // split], j % split * 2 * blk
        copies.append((part.at[:, pl.ds(base, blk), :], q_buf.at[j]))
        copies.append((part.at[:, pl.ds(base + blk, blk), :], kv_buf.at[j, pl.ds(start, blocks)]))
    for j, ref in enumerate((far_ref,) + near):
        copies.append((ref, kv_buf.at[j, pl.ds(blocks - start, blocks)]))
    copies = [pltpu.make_async_copy(a, b, sems.at[i]) for i, (a, b) in enumerate(copies)]
    for copy in copies:
        copy.start()
    order_by_length(lengths_ref, order_ref, lengths_ref.shape[0])
    lane = lax.broadcasted_iota(jnp.int32, (blk, LANES), 1)
    low = lane < HEAD_DIM
    scale = HEAD_DIM ** -0.5
    for copy in copies:
        copy.wait()

    def list_at(j, b):
        return ((j // split * blocks + b) * split + j % split) * LANES

    def head_rows(j, b):
        q = q_buf[j, b].astype(jnp.float32)
        q1 = jnp.where(low, pltpu.roll(q, HEAD_DIM, 1), 0.0)
        q0 = jnp.where(low, q, 0.0)
        return (jnp.concatenate([q0, q1], axis=0) * scale).astype(jnp.bfloat16)

    def body(j, b, length, groups):
        meta = list_at(j, b)
        count = list_ref[meta + stride]
        q2 = head_rows(j, b)
        total = groups * GROUP
        kvs = []
        for t in range(total):
            c = jnp.maximum(list_ref[meta + t], 0)
            kvs.append(kv_buf[j, c])
        kv = jnp.concatenate(kvs, axis=0)
        s = lax.dot_general(q2, kv, (((1,), (1,)), ((), ())), preferred_element_type=jnp.float32)
        row = lax.broadcasted_iota(jnp.int32, (2 * blk, blk), 0) % blk
        col = lax.broadcasted_iota(jnp.int32, (2 * blk, blk), 1)
        parts = []
        for t in range(total):
            part = s[:, t * blk:(t + 1) * blk]
            if t == 0:
                part = jnp.where(col <= row, part, -1e30)
            else:
                part = jnp.where(t < count, part, -1e30)
            parts.append(part)
        peak = parts[0]
        for part in parts[1:]:
            peak = jnp.maximum(peak, part)
        m = jnp.max(peak, axis=1, keepdims=True)
        exps = [jnp.exp(part - m) for part in parts]
        acc = exps[0]
        for e in exps[1:]:
            acc = acc + e
        denom = jnp.sum(acc, axis=1, keepdims=True)
        p = jnp.concatenate([e.astype(jnp.bfloat16) for e in exps], axis=1)
        o = jnp.dot(p, kv, preferred_element_type=jnp.float32) / denom
        o = jnp.where(low, pltpu.roll(o[:blk], HEAD_DIM, 1), o[blk:])
        pos = (start + b) * blk + lax.broadcasted_iota(jnp.int32, (blk, LANES), 0)
        out_ref[b, pl.ds(pl.multiple_of(j * blk, blk), blk), :] = jnp.where(
            pos < length, o, 0.0
        ).astype(jnp.bfloat16)

    @pl.loop(0, slots * blocks // 2)
    def _(step):
        j, b = step // (blocks // 2), step % (blocks // 2) * 2
        rank = j * planes + jnp.where(j % 2 == 0, plane, planes - 1 - plane)
        length = lengths_ref[order_ref[rank]]
        live = (start + b) * blk < length

        @pl.when(live)
        def _():
            need = jnp.maximum(
                list_ref[list_at(j, b) + stride], list_ref[list_at(j, b + 1) + stride]
            )
            for groups in range(1, -(-2 * blocks // GROUP) + 1):
                @pl.when((need > (groups - 1) * GROUP) & (need <= groups * GROUP))
                def _():
                    body(j, b, length, groups)
                    body(j, b + 1, length, groups)

        @pl.when(jnp.logical_not(live))
        def _():
            zero = jnp.zeros((blk, LANES), jnp.bfloat16)
            out_ref[b, pl.ds(pl.multiple_of(j * blk, blk), blk), :] = zero
            out_ref[b + 1, pl.ds(pl.multiple_of(j * blk, blk), blk), :] = zero


def attend(arrived, from_half, lengths, where, lists, split, planes, blk, stride):
    blocks = arrived[0].shape[0]
    slots = split * len(arrived)
    smem = pl.BlockSpec(memory_space=pltpu.SMEM)
    vmem = pl.BlockSpec(memory_space=pltpu.VMEM)
    anywhere = pl.BlockSpec(memory_space=pl.ANY)
    far, *near = from_half
    return pl.pallas_call(
        functools.partial(
            attend_kernel, slots=slots, split=split, planes=planes, blocks=blocks, blk=blk,
            stride=stride,
        ),
        in_specs=[smem, smem, smem] + [anywhere] * (len(from_half) + len(arrived)),
        out_specs=vmem,
        out_shape=jax.ShapeDtypeStruct((blocks, slots * blk, LANES), jnp.bfloat16),
        scratch_shapes=[
            pltpu.SMEM(lengths.shape, jnp.int32),
            pltpu.VMEM((slots, blocks, blk, LANES), jnp.bfloat16),
            pltpu.VMEM((slots, 2 * blocks, blk, LANES), jnp.bfloat16),
            pltpu.SemaphoreType.DMA((2 * slots + len(from_half),)),
        ],
        compiler_params=pltpu.CompilerParams(vmem_limit_bytes=40 << 20),
        cost_estimate=pl.CostEstimate(
            flops=4 * 2 * blk * blk * LANES * blocks * blocks // 2 * slots,
            transcendentals=0,
            bytes_accessed=3 << 20,
        ),
        name="attend",
    )(lengths, where, lists, far, *arrived, *near)


def output_kernel(
    lengths_ref, side_ref, own_ref, other_ref, w_ref, out_ref,
    order_ref, w_buf, rows_buf, sem, out_sems, *, planes, kv_local,
):
    seq_count, blk = out_ref.shape[0], out_ref.shape[1]
    load = pltpu.make_async_copy(w_ref, w_buf, sem)
    load.start()
    order_by_length(lengths_ref, order_ref, seq_count)
    half = kv_local * LANES
    own_at = pl.multiple_of(side_ref[0] * half, half)
    other_at = pl.multiple_of((1 - side_ref[0]) * half, half)

    def rows(ref, rank):
        p, j = place(rank, planes)
        return jnp.concatenate(
            [ref[p * kv_local + h, j * blk:(j + 1) * blk, :] for h in range(kv_local)], axis=1
        )

    load.wait()
    stores = []
    for rank in range(0, seq_count, 2):
        mine = jnp.concatenate([rows(own_ref, rank), rows(own_ref, rank + 1)], axis=0)
        theirs = jnp.concatenate([rows(other_ref, rank), rows(other_ref, rank + 1)], axis=0)
        o = jnp.dot(mine, w_buf[pl.ds(own_at, half), :], preferred_element_type=jnp.float32)
        o = o + jnp.dot(
            theirs, w_buf[pl.ds(other_at, half), :], preferred_element_type=jnp.float32
        )
        rows_buf[rank:rank + 2] = o.astype(jnp.bfloat16).reshape(2, blk, -1)
        for r in (rank, rank + 1):
            store = pltpu.make_async_copy(
                rows_buf.at[r], out_ref.at[order_ref[r]], out_sems.at[r]
            )
            store.start()
            stores.append(store)
    for store in stores:
        store.wait()


def output_projection(own, other, w_output, lengths, side, planes, kv_local, blk):
    seq_count = lengths.shape[0]
    width = w_output.shape[1]
    smem = pl.BlockSpec(memory_space=pltpu.SMEM)
    vmem = pl.BlockSpec(memory_space=pltpu.VMEM)
    hbm = pl.BlockSpec(memory_space=HBM)
    return pl.pallas_call(
        functools.partial(output_kernel, planes=planes, kv_local=kv_local),
        in_specs=[smem, smem, vmem, vmem, hbm],
        out_specs=hbm,
        out_shape=jax.ShapeDtypeStruct((seq_count, blk, width), jnp.bfloat16),
        scratch_shapes=[
            pltpu.SMEM((seq_count,), jnp.int32),
            pltpu.VMEM(w_output.shape, jnp.bfloat16),
            pltpu.VMEM((seq_count, blk, width), jnp.bfloat16),
            pltpu.SemaphoreType.DMA,
            pltpu.SemaphoreType.DMA((seq_count,)),
        ],
        compiler_params=pltpu.CompilerParams(vmem_limit_bytes=40 << 20),
        cost_estimate=pl.CostEstimate(
            flops=2 * seq_count * blk * w_output.size, transcendentals=0, bytes_accessed=6 << 20
        ),
        name="output_projection",
    )(lengths, side, own, other, w_output)


def place(rank, planes):
    j, step = divmod(rank, planes)
    return (step if j % 2 == 0 else planes - 1 - step), j


def per_device(tokens, w_query, w_key, w_value, w_output, chosen, lengths):
    seq_count, blk, _ = tokens.shape
    kv_devices = lax.axis_size("kv")
    kv_local = w_key.shape[1] // HEAD_DIM
    half = kv_devices // 2
    planes = half // kv_local
    slots = seq_count // planes
    split = slots // 2
    select = chosen.shape[2]
    ranks = {place(rank, planes): rank for rank in range(seq_count)}
    groups = [
        tuple(ranks[p, part * split + j] for p in range(planes) for j in range(split))
        for part in range(2)
    ]
    halves = [list(range(half)), list(range(half, kv_devices))]

    def exchange(x):
        return lax.all_to_all(
            x, "kv", split_axis=0, concat_axis=0, tiled=True, axis_index_groups=halves
        )

    def lists_of(arrived):
        at = split * 2 * blk
        return arrived[:, at:at + split, :].astype(jnp.int32)

    def to_second_half(x):
        return lax.ppermute(x, "kv", [(i, i + half) for i in range(half)])

    here = lax.axis_index("kv").astype(jnp.int32)
    where = jnp.stack([here % half // kv_local, here // half * half])
    sent_a = project(tokens, w_query, w_key, w_value, chosen, lengths, groups[0], split, kv_local)
    arrived_a = exchange(sent_a)
    later, _ = lax.optimization_barrier((lengths, sent_a))
    sent_b = project(tokens, w_query, w_key, w_value, chosen, later, groups[1], split, kv_local)
    from_half = []
    for j in range(split):
        kv = arrived_a[:, (2 * j + 1) * blk:(2 * j + 2) * blk, :]
        if j == 0:
            from_half.append(to_second_half(kv))
        else:
            longer = jnp.sum((lengths > half * blk).astype(jnp.int32)) > j * planes
            from_half.append(lax.cond(longer, to_second_half, lambda x: x, kv))
    arrived_b = exchange(sent_b)
    lists = jnp.concatenate([lists_of(arrived_a), lists_of(arrived_b)]).reshape(-1)
    attended = attend(
        [arrived_a, arrived_b], from_half, lengths, where, lists, split, planes, blk, select
    )
    own = exchange(attended)
    other = lax.ppermute(own, "tp", [(0, 1), (1, 0)])
    side = lax.axis_index("tp").astype(jnp.int32)[None]
    return output_projection(own, other, w_output, lengths, side, planes, kv_local, blk)


def fits(mesh, tokens, w_key, chosen):
    seq_count, seq_len = tokens.shape[0], tokens.shape[1]
    kv_devices, tp_devices = mesh.shape["kv"], mesh.shape["tp"]
    kv_local = w_key.shape[1] // tp_devices // HEAD_DIM
    if HEADS // KV_HEADS * HEAD_DIM != LANES or 2 * HEAD_DIM != LANES or tp_devices != 2:
        return False
    if kv_local == 0 or kv_devices % (4 * kv_local) or kv_devices > 16 or chosen.shape[2] >= LANES:
        return False
    planes = kv_devices // 2 // kv_local
    if seq_len // kv_devices != LANES or seq_count % (2 * planes) or seq_count % 4:
        return False
    split = seq_count // planes // 2
    fits_half = (seq_count - 1) * seq_len // 4 // (split * planes) <= seq_len // 2
    return split <= META_ROWS and planes * split % 2 == 0 and fits_half


def fits(mesh, tokens, w_key, chosen):
    seq_count, seq_len = tokens.shape[0], tokens.shape[1]
    kv_devices, tp_devices = mesh.shape["kv"], mesh.shape["tp"]
    kv_local = w_key.shape[1] // tp_devices // HEAD_DIM
    if HEADS // KV_HEADS * HEAD_DIM != LANES or 2 * HEAD_DIM != LANES or tp_devices != 2:
        return False
    if kv_local == 0 or kv_devices % (4 * kv_local) or kv_devices > 16 or chosen.shape[2] >= LANES:
        return False
    planes = kv_devices // kv_local
    if seq_len // kv_devices != LANES or seq_count <= planes or seq_count % 2 or planes % 2:
        return False
    slots, odd = divmod(seq_count - planes, planes // 2)
    fits_half = (seq_count - 1) * seq_len // 4 // planes <= seq_len // 2
    return odd == 0 and slots <= META_ROWS and (planes // 2 * slots) % 2 == 0 and fits_half


def solution(mesh):
    def run(tokens, w_query, w_key, w_value, w_output, chosen, lengths):
        body = per_device if fits(mesh, tokens, w_key, chosen) else per_device_general
        return jax.shard_map(
            body,
            mesh=mesh,
            in_specs=(
                P(None, "kv", None),
                P(None, "tp"),
                P(None, "tp"),
                P(None, "tp"),
                P(None, "tp"),
                P(None, "kv", None),
                P(),
            ),
            out_specs=P(None, "kv", "tp"),
            check_vma=False,
        )(tokens, w_query, w_key, w_value, w_output, chosen, lengths)

    return run
```

```python
import functools

import jax
import jax.numpy as jnp
from jax import lax
from jax.experimental import pallas as pl
from jax.experimental.pallas import tpu as pltpu
from jax.sharding import PartitionSpec as P


HEADS = 16
KV_HEADS = 8
HEAD_DIM = 64
CAP = 4
META_ROWS = 16
LANES = 128
VMEM_MOST = 63 << 20
HBM = pltpu.HBM


def per_device_general(tokens, w_query, w_key, w_value, w_output, chosen, lengths):
    seq_count, block_len, model_width = tokens.shape
    flat_rows = tokens.reshape(seq_count * block_len, model_width)
    queries = jnp.dot(flat_rows, w_query, preferred_element_type=jnp.float32).astype(jnp.bfloat16)
    key_proj = jnp.dot(flat_rows, w_key, preferred_element_type=jnp.float32).astype(jnp.bfloat16)
    value_proj = jnp.dot(flat_rows, w_value, preferred_element_type=jnp.float32).astype(
        jnp.bfloat16
    )
    key_width = key_proj.shape[1]
    local_blocks = jnp.concatenate([key_proj, value_proj], axis=1).reshape(
        seq_count, block_len, 2 * key_width
    )
    shard_member = lax.axis_index("kv")
    kv_devices = lax.axis_size("kv")
    picked = chosen[:, 0, :]
    clipped = jnp.maximum(picked, 0)
    seq_index = jnp.arange(seq_count, dtype=jnp.int32)
    owners = jnp.arange(kv_devices, dtype=jnp.int32)
    wanted = (
        jnp.any(picked[:, :, None] == owners[None, None, :], axis=1)
        & (owners != shard_member)[None, :]
    )
    wanted = wanted.T
    ranked = jnp.cumsum(wanted.astype(jnp.int32), axis=1) - 1
    slot_hit = wanted[:, :, None] & (
        ranked[:, :, None] == jnp.arange(CAP, dtype=jnp.int32)[None, None, :]
    )
    request = jnp.sum(slot_hit.astype(jnp.int32) * (seq_index + 1)[None, :, None], axis=1) - 1
    incoming = lax.all_to_all(request, "kv", split_axis=0, concat_axis=0, tiled=True)
    outgoing = local_blocks[jnp.maximum(incoming, 0)]
    arrived = lax.all_to_all(outgoing, "kv", split_axis=0, concat_axis=0, tiled=True)
    key_lookup = jnp.concatenate(
        [local_blocks, arrived.reshape(kv_devices * CAP, block_len, 2 * key_width)], axis=0
    )
    rank_at = jnp.take_along_axis(ranked.T, clipped, axis=1)
    source = jnp.where(
        picked == shard_member, seq_index[:, None], seq_count + clipped * CAP + rank_at
    )
    group_size = HEADS // KV_HEADS
    local_kv_heads = key_width // HEAD_DIM
    query_pos = shard_member * block_len + jnp.arange(block_len, dtype=jnp.int32)
    score_scale = HEAD_DIM ** (-0.5)

    def attend(packed):
        query_rows, source_row, pick_row, length = packed
        fetched = key_lookup[source_row]
        slot_count = pick_row.shape[0]
        key_rows = fetched[:, :, :key_width].reshape(
            slot_count * block_len, local_kv_heads, HEAD_DIM
        )
        value_rows = fetched[:, :, key_width:].reshape(
            slot_count * block_len, local_kv_heads, HEAD_DIM
        )
        grouped = query_rows.reshape(block_len, local_kv_heads, group_size, HEAD_DIM)
        scores = (
            jnp.einsum("qkgd,nkd->kgqn", grouped, key_rows, preferred_element_type=jnp.float32)
            * score_scale
        )
        key_pos = (
            pick_row[:, None] * block_len + jnp.arange(block_len, dtype=jnp.int32)[None, :]
        ).reshape(-1)
        listed = jnp.repeat(pick_row >= 0, block_len)
        allowed = (
            listed[None, :] & (key_pos[None, :] <= query_pos[:, None]) & (key_pos[None, :] < length)
        )
        masked = jnp.where(allowed, scores, -1e30)
        row_max = jnp.max(masked, axis=-1, keepdims=True)
        exponent = jnp.exp(masked - row_max)
        weights = (exponent / jnp.sum(exponent, axis=-1, keepdims=True)).astype(jnp.bfloat16)
        mixed_heads = jnp.einsum(
            "kgqn,nkd->qkgd", weights, value_rows, preferred_element_type=jnp.float32
        )
        live_rows = (query_pos < length)[:, None, None, None]
        return jnp.where(live_rows, mixed_heads, 0.0).astype(jnp.bfloat16).reshape(block_len, -1)

    attended = lax.map(attend, (queries.reshape(seq_count, block_len, -1), source, picked, lengths))
    attended_rows = attended.reshape(seq_count * block_len, -1)
    summed = jnp.dot(
        lax.all_gather(attended_rows, "tp", axis=1, tiled=True),
        w_output,
        preferred_element_type=jnp.float32,
    )
    return summed.astype(jnp.bfloat16).reshape(seq_count, block_len, -1)


def order_by_length(lengths_ref, order_ref, seq_count):
    for s in range(seq_count):
        rank = jnp.int32(0)
        for t in range(seq_count):
            if t < s:
                ahead = lengths_ref[t] >= lengths_ref[s]
            elif t > s:
                ahead = lengths_ref[t] > lengths_ref[s]
            else:
                continue
            rank = rank + jnp.where(ahead, 1, 0)
        order_ref[rank] = s


def project_kernel(
    lengths_in, chosen_in, tokens_ref, wq_ref, wk_ref, wv_ref, out_ref,
    lengths_ref, chosen_ref, order_ref, meta_ref, rows_ref, wq_buf, wk_buf, wv_buf, row_sems, w_sems,
    *, ranks, slots, kv_local, select,
):
    seq_count = chosen_ref.shape[0]
    blk = tokens_ref.shape[1]
    loads = [
        pltpu.make_async_copy(wq_ref, wq_buf, w_sems.at[0]),
        pltpu.make_async_copy(wk_ref, wk_buf, w_sems.at[1]),
        pltpu.make_async_copy(wv_ref, wv_buf, w_sems.at[2]),
    ]
    small = [
        pltpu.make_async_copy(lengths_in, lengths_ref, w_sems.at[3]),
        pltpu.make_async_copy(chosen_in, chosen_ref, w_sems.at[4]),
    ]
    for load in small + loads[1:]:
        load.start()
    small[0].wait()
    order_by_length(lengths_ref, order_ref, seq_count)
    fetch = [
        pltpu.make_async_copy(
            tokens_ref.at[order_ref[rank]], rows_ref.at[pl.ds(i * blk, blk)], row_sems.at[i]
        )
        for i, rank in enumerate(ranks)
    ]
    for f in fetch[:2] + loads[:1] + fetch[2:]:
        f.start()
    small[1].wait()
    meta_ref[...] = jnp.zeros(meta_ref.shape, jnp.float32)
    for s in range(seq_count):
        meta_ref[s:s + 1, :select] = chosen_ref[s].astype(jnp.float32)
    lane = lax.broadcasted_iota(jnp.int32, meta_ref.shape, 1)
    named = meta_ref[...]
    count = jnp.sum(jnp.where((lane < select) & (named >= 0), 1.0, 0.0), axis=1, keepdims=True)
    meta_ref[...] = jnp.where(lane == select, count, named)
    tile_row = lax.broadcasted_iota(jnp.int32, (META_ROWS, LANES), 0)
    planes = len(ranks) // slots
    for p in range(planes):
        tile = jnp.zeros((META_ROWS, LANES), jnp.float32)
        for j in range(slots):
            row = meta_ref[pl.ds(order_ref[ranks[p * slots + j]], 1), :]
            tile = jnp.where(tile_row == j, row, tile)
        tile = tile.astype(jnp.bfloat16)
        for h in range(kv_local):
            out_ref[p * kv_local + h, slots * 2 * blk:, :] = tile
    for first in range(0, len(ranks), 2):
        fetch[first].wait()
        fetch[first + 1].wait()
        rows = rows_ref[first * blk:(first + 2) * blk, :]
        if first == 0:
            loads[1].wait()
            loads[2].wait()
        k = jnp.dot(rows, wk_buf[...], preferred_element_type=jnp.float32).astype(jnp.bfloat16)
        v = jnp.dot(rows, wv_buf[...], preferred_element_type=jnp.float32).astype(jnp.bfloat16)
        if first == 0:
            loads[0].wait()
        q = jnp.dot(rows, wq_buf[...], preferred_element_type=jnp.float32).astype(jnp.bfloat16)
        for h in range(kv_local):
            q_h = q[:, h * LANES:(h + 1) * LANES]
            kv_h = jnp.concatenate(
                [k[:, h * HEAD_DIM:(h + 1) * HEAD_DIM], v[:, h * HEAD_DIM:(h + 1) * HEAD_DIM]],
                axis=1,
            )
            for i in range(2):
                p, j = divmod(first + i, slots)
                base = j * 2 * blk
                out_ref[p * kv_local + h, base:base + blk, :] = q_h[i * blk:(i + 1) * blk]
                out_ref[p * kv_local + h, base + blk:base + 2 * blk, :] = kv_h[i * blk:(i + 1) * blk]


def project(tokens, w_query, w_key, w_value, chosen, lengths, ranks, slots, kv_local):
    seq_count, blk, width = tokens.shape
    dests = len(ranks) // slots * kv_local
    rows = slots * 2 * blk + META_ROWS
    hbm = pl.BlockSpec(memory_space=HBM)
    return pl.pallas_call(
        functools.partial(
            project_kernel, ranks=ranks, slots=slots, kv_local=kv_local, select=chosen.shape[2]
        ),
        in_specs=[hbm] * 6,
        out_specs=pl.BlockSpec(memory_space=pltpu.VMEM),
        out_shape=jax.ShapeDtypeStruct((dests, rows, LANES), jnp.bfloat16),
        scratch_shapes=[
            pltpu.SMEM((seq_count,), jnp.int32),
            pltpu.VMEM(chosen.shape, jnp.int32),
            pltpu.SMEM((seq_count,), jnp.int32),
            pltpu.VMEM((seq_count, LANES), jnp.float32),
            pltpu.VMEM((len(ranks) * blk, width), jnp.bfloat16),
            pltpu.VMEM(w_query.shape, jnp.bfloat16),
            pltpu.VMEM(w_key.shape, jnp.bfloat16),
            pltpu.VMEM(w_value.shape, jnp.bfloat16),
            pltpu.SemaphoreType.DMA((len(ranks),)),
            pltpu.SemaphoreType.DMA((5,)),
        ],
        compiler_params=pltpu.CompilerParams(vmem_limit_bytes=VMEM_MOST),
        cost_estimate=pl.CostEstimate(
            flops=2 * len(ranks) * blk * width * 2 * kv_local * LANES,
            transcendentals=0,
            bytes_accessed=2 * (len(ranks) * blk * width + w_query.size * 2 + dests * rows * LANES),
        ),
        name="project",
    )(lengths, chosen, tokens, w_query, w_key, w_value)


def attend_kernel(
    lengths_ref, where_ref, list_ref, *refs, early, split, planes, blocks, blk, stride, sizes,
):
    plane, start = where_ref[0], where_ref[1]
    first_half = start == 0
    if early:
        arrived, out_ref, order_ref, q_buf, kv_buf, o_buf, sems, out_sem = refs
        part = 0
    else:
        own, arrived = refs[0], refs[1]
        far = refs[2:2 + split]
        out_ref, order_ref, q_buf, kv_buf, o_buf, sems, out_sem = refs[3 + split:]
        part = jnp.where(first_half, 1, 0)

    def loads(source, remote):
        pairs = []
        for j in range(split):
            base = j * 2 * blk
            pairs.append((source.at[:, pl.ds(base, blk), :], q_buf.at[j]))
            at = kv_buf.at[j, pl.ds(blocks if remote else 0, blocks)]
            pairs.append((source.at[:, pl.ds(base + blk, blk), :], at))
            if remote:
                pairs.append((far[j], kv_buf.at[j, pl.ds(0, blocks)]))
        return [pltpu.make_async_copy(a, b, sems.at[i]) for i, (a, b) in enumerate(pairs)]

    def fetch(source, remote):
        copies = loads(source, remote)
        for copy in copies:
            copy.start()
        for copy in copies:
            copy.wait()

    lane = lax.broadcasted_iota(jnp.int32, (blk, LANES), 1)
    low = lane < HEAD_DIM
    row = lax.broadcasted_iota(jnp.int32, (2 * blk, blk), 0) % blk
    col = lax.broadcasted_iota(jnp.int32, (2 * blk, blk), 1)
    scale = HEAD_DIM ** -0.5

    def list_at(j, b):
        kind = 0 if early else part * blocks
        return ((kind + b) * split + j) * LANES

    def head_rows(j, b):
        q = q_buf[j, b].astype(jnp.float32)
        q1 = jnp.where(low, pltpu.roll(q, HEAD_DIM, 1), 0.0)
        q0 = jnp.where(low, q, 0.0)
        return (jnp.concatenate([q0, q1], axis=0) * scale).astype(jnp.bfloat16)

    def body(j, b, length, total):
        meta = list_at(j, b)
        count = list_ref[meta + stride]
        q2 = head_rows(j, b)
        kv = jnp.concatenate(
            [kv_buf[j, jnp.maximum(list_ref[meta + t], 0)] for t in range(total)], axis=0
        )
        s = lax.dot_general(q2, kv, (((1,), (1,)), ((), ())), preferred_element_type=jnp.float32)
        parts = []
        for t in range(total):
            piece = s[:, t * blk:(t + 1) * blk]
            if t == 0:
                piece = jnp.where(col <= row, piece, -1e30)
            else:
                piece = jnp.where(t < count, piece, -1e30)
            parts.append(piece)
        peak = parts[0]
        for piece in parts[1:]:
            peak = jnp.maximum(peak, piece)
        m = jnp.max(peak, axis=1, keepdims=True)
        p = jnp.concatenate([jnp.exp(piece - m).astype(jnp.bfloat16) for piece in parts], axis=1)
        low_rows = lax.broadcasted_iota(jnp.int32, kv.shape, 1) < HEAD_DIM
        values = jnp.where(low_rows, jnp.ones_like(kv), kv)
        o = jnp.dot(p, values, preferred_element_type=jnp.float32)
        turned = pltpu.roll(o, HEAD_DIM, 1)
        o = jnp.where(low, turned[:blk] / o[:blk], o[blk:] / turned[blk:])
        pos = (start + b) * blk + lax.broadcasted_iota(jnp.int32, (blk, LANES), 0)
        o_buf[b, pl.ds(pl.multiple_of(j * blk, blk), blk), :] = jnp.where(
            pos < length, o, 0.0
        ).astype(jnp.bfloat16)

    def run():
        order_by_length(lengths_ref, order_ref, lengths_ref.shape[0])

        @pl.loop(0, split * blocks // 2)
        def _(step):
            j, b = step // (blocks // 2), step % (blocks // 2) * 2
            slot = part * split + j
            rank = slot * planes + jnp.where(slot % 2 == 0, plane, planes - 1 - plane)
            length = lengths_ref[order_ref[rank]]
            need = jnp.maximum(
                list_ref[list_at(j, b) + stride], list_ref[list_at(j, b + 1) + stride]
            )
            live = (start + b) * blk < length
            less = 0
            for size in sizes:
                @pl.when(live & (need > less) & (need <= size))
                def _():
                    body(j, b, length, size)
                    body(j, b + 1, length, size)

                less = size

        at = pl.ds(0 if early else pl.multiple_of(part * split * blk, split * blk), split * blk)
        store = pltpu.make_async_copy(o_buf, out_ref.at[:, at, :], out_sem)
        store.start()
        store.wait()

    if early:
        @pl.when(first_half)
        def _():
            fetch(arrived, False)
            run()
    else:
        @pl.when(first_half)
        def _():
            fetch(arrived, False)

        @pl.when(jnp.logical_not(first_half))
        def _():
            fetch(own, True)

        run()


def attend(lengths, where, lists, operands, early, split, planes, blk, stride):
    blocks = operands[0].shape[0]
    smem = pl.BlockSpec(memory_space=pltpu.SMEM)
    anywhere = pl.BlockSpec(memory_space=pl.ANY)
    most = blocks if early else 2 * blocks
    sizes = tuple(n for n in (2, 4, 6, 8, 10, 12, 16) if n < most) + (most,)
    return pl.pallas_call(
        functools.partial(
            attend_kernel, early=early, split=split, planes=planes, blocks=blocks, blk=blk,
            stride=stride, sizes=sizes,
        ),
        in_specs=[smem, smem, smem] + [anywhere] * len(operands),
        out_specs=anywhere,
        out_shape=jax.ShapeDtypeStruct((blocks, 2 * split * blk, LANES), jnp.bfloat16),
        scratch_shapes=[
            pltpu.SMEM(lengths.shape, jnp.int32),
            pltpu.VMEM((split, blocks, blk, LANES), jnp.bfloat16),
            pltpu.VMEM((split, most, blk, LANES), jnp.bfloat16),
            pltpu.VMEM((blocks, split * blk, LANES), jnp.bfloat16),
            pltpu.SemaphoreType.DMA((3 * split,)),
            pltpu.SemaphoreType.DMA,
        ],
        input_output_aliases={} if early else {2 + len(operands): 0},
        compiler_params=pltpu.CompilerParams(vmem_limit_bytes=40 << 20),
        cost_estimate=pl.CostEstimate(
            flops=4 * 2 * blk * blk * LANES * blocks * blocks * split,
            transcendentals=0,
            bytes_accessed=3 << 20,
        ),
        name="attend_early" if early else "attend",
    )(lengths, where, lists, *operands)


def output_kernel(
    lengths_ref, side_ref, own_ref, other_ref, w_ref, out_ref,
    order_ref, w_buf, rows_buf, sem, out_sems, *, planes, kv_local,
):
    seq_count, blk = out_ref.shape[0], out_ref.shape[1]
    load = pltpu.make_async_copy(w_ref, w_buf, sem)
    load.start()
    order_by_length(lengths_ref, order_ref, seq_count)
    half = kv_local * LANES
    own_at = pl.multiple_of(side_ref[0] * half, half)
    other_at = pl.multiple_of((1 - side_ref[0]) * half, half)

    def rows(ref, rank):
        p, j = place(rank, planes)
        return jnp.concatenate(
            [ref[p * kv_local + h, j * blk:(j + 1) * blk, :] for h in range(kv_local)], axis=1
        )

    load.wait()
    stores = []
    for rank in range(0, seq_count, 2):
        mine = jnp.concatenate([rows(own_ref, rank), rows(own_ref, rank + 1)], axis=0)
        theirs = jnp.concatenate([rows(other_ref, rank), rows(other_ref, rank + 1)], axis=0)
        o = jnp.dot(mine, w_buf[pl.ds(own_at, half), :], preferred_element_type=jnp.float32)
        o = o + jnp.dot(
            theirs, w_buf[pl.ds(other_at, half), :], preferred_element_type=jnp.float32
        )
        for r in (rank, rank + 1):
            live = side_ref[1] < lengths_ref[order_ref[r]]
            rows_buf[r] = jnp.where(
                live, o[(r - rank) * blk:(r - rank + 1) * blk], 0.0
            ).astype(jnp.bfloat16)
            store = pltpu.make_async_copy(
                rows_buf.at[r], out_ref.at[order_ref[r]], out_sems.at[r]
            )
            store.start()
            stores.append(store)
    for store in stores:
        store.wait()


def output_projection(own, other, w_output, lengths, side, planes, kv_local, blk):
    seq_count = lengths.shape[0]
    width = w_output.shape[1]
    smem = pl.BlockSpec(memory_space=pltpu.SMEM)
    vmem = pl.BlockSpec(memory_space=pltpu.VMEM)
    hbm = pl.BlockSpec(memory_space=HBM)
    return pl.pallas_call(
        functools.partial(output_kernel, planes=planes, kv_local=kv_local),
        in_specs=[smem, smem, vmem, vmem, hbm],
        out_specs=hbm,
        out_shape=jax.ShapeDtypeStruct((seq_count, blk, width), jnp.bfloat16),
        scratch_shapes=[
            pltpu.SMEM((seq_count,), jnp.int32),
            pltpu.VMEM(w_output.shape, jnp.bfloat16),
            pltpu.VMEM((seq_count, blk, width), jnp.bfloat16),
            pltpu.SemaphoreType.DMA,
            pltpu.SemaphoreType.DMA((seq_count,)),
        ],
        compiler_params=pltpu.CompilerParams(vmem_limit_bytes=40 << 20),
        cost_estimate=pl.CostEstimate(
            flops=2 * seq_count * blk * w_output.size, transcendentals=0, bytes_accessed=6 << 20
        ),
        name="output_projection",
    )(lengths, side, own, other, w_output)


def place(rank, planes):
    j, step = divmod(rank, planes)
    return (step if j % 2 == 0 else planes - 1 - step), j


def per_device(tokens, w_query, w_key, w_value, w_output, chosen, lengths):
    seq_count, blk, _ = tokens.shape
    kv_devices = lax.axis_size("kv")
    kv_local = w_key.shape[1] // HEAD_DIM
    half = kv_devices // 2
    planes = half // kv_local
    slots = seq_count // planes
    split = slots // 2
    select = chosen.shape[2]
    ranks = {place(rank, planes): rank for rank in range(seq_count)}
    groups = [
        tuple(ranks[p, part * split + j] for p in range(planes) for j in range(split))
        for part in range(2)
    ]
    halves = [list(range(half)), list(range(half, kv_devices))]

    def exchange(x):
        return lax.all_to_all(
            x, "kv", split_axis=0, concat_axis=0, tiled=True, axis_index_groups=halves
        )

    def lists_of(arrived):
        at = split * 2 * blk
        return arrived[:, at:at + split, :].astype(jnp.int32)

    def to_second_half(x):
        return lax.ppermute(x, "kv", [(i, i + half) for i in range(half)])

    here = lax.axis_index("kv").astype(jnp.int32)
    where = jnp.stack([here % half // kv_local, here // half * half])
    sent_a = project(tokens, w_query, w_key, w_value, chosen, lengths, groups[0], split, kv_local)
    arrived_a = exchange(sent_a)
    later, _ = lax.optimization_barrier((lengths, sent_a))
    sent_b = project(tokens, w_query, w_key, w_value, chosen, later, groups[1], split, kv_local)
    lists_a = lists_of(arrived_a)
    started = attend(
        lengths, where, lists_a.reshape(-1), [arrived_a], True, split, planes, blk, select
    )

    def keys_of(arrived, j):
        return arrived[:, (2 * j + 1) * blk:(2 * j + 2) * blk, :]

    from_half = [to_second_half(keys_of(arrived_a, 0))]
    for j in range(1, split):
        longer = jnp.sum((lengths > half * blk).astype(jnp.int32)) > j * planes
        from_half.append(
            lax.cond(
                longer,
                lambda x: to_second_half(keys_of(x, j)),
                lambda x: jnp.zeros((half, blk, LANES), x.dtype),
                arrived_a,
            )
        )
    arrived_b = exchange(sent_b)
    lists = jnp.concatenate([lists_a, lists_of(arrived_b)]).reshape(-1)
    attended = attend(
        lengths, where, lists, [arrived_a, arrived_b] + from_half + [started], False, split,
        planes, blk, select,
    )
    own = exchange(attended)
    other = lax.ppermute(own, "tp", [(0, 1), (1, 0)])
    side = jnp.stack([lax.axis_index("tp").astype(jnp.int32), here * blk])
    return output_projection(own, other, w_output, lengths, side, planes, kv_local, blk)


def fits(mesh, tokens, w_key, chosen):
    seq_count, seq_len = tokens.shape[0], tokens.shape[1]
    kv_devices, tp_devices = mesh.shape["kv"], mesh.shape["tp"]
    kv_local = w_key.shape[1] // tp_devices // HEAD_DIM
    if HEADS // KV_HEADS * HEAD_DIM != LANES or 2 * HEAD_DIM != LANES or tp_devices != 2:
        return False
    if kv_local == 0 or kv_devices % (4 * kv_local) or kv_devices > 16 or chosen.shape[2] >= LANES:
        return False
    planes = kv_devices // 2 // kv_local
    if seq_len // kv_devices != LANES or seq_count % (2 * planes) or seq_count % 4:
        return False
    split = seq_count // planes // 2
    fits_half = (seq_count - 1) * seq_len // 4 // (split * planes) <= seq_len // 2
    return split <= META_ROWS and planes * split % 2 == 0 and fits_half


def fits(mesh, tokens, w_key, chosen):
    seq_count, seq_len = tokens.shape[0], tokens.shape[1]
    kv_devices, tp_devices = mesh.shape["kv"], mesh.shape["tp"]
    kv_local = w_key.shape[1] // tp_devices // HEAD_DIM
    if HEADS // KV_HEADS * HEAD_DIM != LANES or 2 * HEAD_DIM != LANES or tp_devices != 2:
        return False
    if kv_local == 0 or kv_devices % (4 * kv_local) or kv_devices > 16 or chosen.shape[2] >= LANES:
        return False
    planes = kv_devices // kv_local
    if seq_len // kv_devices != LANES or seq_count <= planes or seq_count % 2 or planes % 2:
        return False
    slots, odd = divmod(seq_count - planes, planes // 2)
    fits_half = (seq_count - 1) * seq_len // 4 // planes <= seq_len // 2
    return odd == 0 and slots <= META_ROWS and (planes // 2 * slots) % 2 == 0 and fits_half


def solution(mesh):
    def run(tokens, w_query, w_key, w_value, w_output, chosen, lengths):
        def sharded(body):
            return jax.shard_map(
                body,
                mesh=mesh,
                in_specs=(
                    P(None, "kv", None),
                    P(None, "tp"),
                    P(None, "tp"),
                    P(None, "tp"),
                    P(None, "tp"),
                    P(None, "kv", None),
                    P(),
                ),
                out_specs=P(None, "kv", "tp"),
                check_vma=False,
            )

        arrays = (tokens, w_query, w_key, w_value, w_output, chosen, lengths)
        if not fits(mesh, tokens, w_key, chosen):
            return sharded(per_device_general)(*arrays)

        return sharded(per_device)(*arrays)

    return run
```

```python
import functools

import jax
import jax.numpy as jnp
from jax import lax
from jax.experimental import pallas as pl
from jax.experimental.pallas import tpu as pltpu
from jax.sharding import PartitionSpec as P


HEADS = 16
KV_HEADS = 8
HEAD_DIM = 64
CAP = 4
META_ROWS = 16
LANES = 128
HBM = pltpu.HBM


def per_device_general(tokens, w_query, w_key, w_value, w_output, chosen, lengths):
    seq_count, block_len, model_width = tokens.shape
    flat_rows = tokens.reshape(seq_count * block_len, model_width)
    queries = jnp.dot(flat_rows, w_query, preferred_element_type=jnp.float32).astype(jnp.bfloat16)
    key_proj = jnp.dot(flat_rows, w_key, preferred_element_type=jnp.float32).astype(jnp.bfloat16)
    value_proj = jnp.dot(flat_rows, w_value, preferred_element_type=jnp.float32).astype(
        jnp.bfloat16
    )
    key_width = key_proj.shape[1]
    local_blocks = jnp.concatenate([key_proj, value_proj], axis=1).reshape(
        seq_count, block_len, 2 * key_width
    )
    shard_member = lax.axis_index("kv")
    kv_devices = lax.axis_size("kv")
    picked = chosen[:, 0, :]
    clipped = jnp.maximum(picked, 0)
    seq_index = jnp.arange(seq_count, dtype=jnp.int32)
    owners = jnp.arange(kv_devices, dtype=jnp.int32)
    wanted = (
        jnp.any(picked[:, :, None] == owners[None, None, :], axis=1)
        & (owners != shard_member)[None, :]
    )
    wanted = wanted.T
    ranked = jnp.cumsum(wanted.astype(jnp.int32), axis=1) - 1
    slot_hit = wanted[:, :, None] & (
        ranked[:, :, None] == jnp.arange(CAP, dtype=jnp.int32)[None, None, :]
    )
    request = jnp.sum(slot_hit.astype(jnp.int32) * (seq_index + 1)[None, :, None], axis=1) - 1
    incoming = lax.all_to_all(request, "kv", split_axis=0, concat_axis=0, tiled=True)
    outgoing = local_blocks[jnp.maximum(incoming, 0)]
    arrived = lax.all_to_all(outgoing, "kv", split_axis=0, concat_axis=0, tiled=True)
    key_lookup = jnp.concatenate(
        [local_blocks, arrived.reshape(kv_devices * CAP, block_len, 2 * key_width)], axis=0
    )
    rank_at = jnp.take_along_axis(ranked.T, clipped, axis=1)
    source = jnp.where(
        picked == shard_member, seq_index[:, None], seq_count + clipped * CAP + rank_at
    )
    group_size = HEADS // KV_HEADS
    local_kv_heads = key_width // HEAD_DIM
    query_pos = shard_member * block_len + jnp.arange(block_len, dtype=jnp.int32)
    score_scale = HEAD_DIM ** (-0.5)

    def attend(packed):
        query_rows, source_row, pick_row, length = packed
        fetched = key_lookup[source_row]
        slot_count = pick_row.shape[0]
        key_rows = fetched[:, :, :key_width].reshape(
            slot_count * block_len, local_kv_heads, HEAD_DIM
        )
        value_rows = fetched[:, :, key_width:].reshape(
            slot_count * block_len, local_kv_heads, HEAD_DIM
        )
        grouped = query_rows.reshape(block_len, local_kv_heads, group_size, HEAD_DIM)
        scores = (
            jnp.einsum("qkgd,nkd->kgqn", grouped, key_rows, preferred_element_type=jnp.float32)
            * score_scale
        )
        key_pos = (
            pick_row[:, None] * block_len + jnp.arange(block_len, dtype=jnp.int32)[None, :]
        ).reshape(-1)
        listed = jnp.repeat(pick_row >= 0, block_len)
        allowed = (
            listed[None, :] & (key_pos[None, :] <= query_pos[:, None]) & (key_pos[None, :] < length)
        )
        masked = jnp.where(allowed, scores, -1e30)
        row_max = jnp.max(masked, axis=-1, keepdims=True)
        exponent = jnp.exp(masked - row_max)
        weights = (exponent / jnp.sum(exponent, axis=-1, keepdims=True)).astype(jnp.bfloat16)
        mixed_heads = jnp.einsum(
            "kgqn,nkd->qkgd", weights, value_rows, preferred_element_type=jnp.float32
        )
        live_rows = (query_pos < length)[:, None, None, None]
        return jnp.where(live_rows, mixed_heads, 0.0).astype(jnp.bfloat16).reshape(block_len, -1)

    attended = lax.map(attend, (queries.reshape(seq_count, block_len, -1), source, picked, lengths))
    attended_rows = attended.reshape(seq_count * block_len, -1)
    summed = jnp.dot(
        lax.all_gather(attended_rows, "tp", axis=1, tiled=True),
        w_output,
        preferred_element_type=jnp.float32,
    )
    return summed.astype(jnp.bfloat16).reshape(seq_count, block_len, -1)


def order_by_length(lengths_ref, order_ref, seq_count):
    for s in range(seq_count):
        rank = jnp.int32(0)
        for t in range(seq_count):
            if t < s:
                ahead = lengths_ref[t] >= lengths_ref[s]
            elif t > s:
                ahead = lengths_ref[t] > lengths_ref[s]
            else:
                continue
            rank = rank + jnp.where(ahead, 1, 0)
        order_ref[rank] = s


def project_kernel(
    lengths_in, chosen_in, tokens_ref, wq_ref, wk_ref, wv_ref, sent_ref,
    out_ref, sent_sems, lengths_ref, chosen_ref, order_ref, meta_ref, rows_ref, wq_buf, wk_buf, wv_buf, row_sems, w_sems,
    *, ranks, slots, kv_local, select,
):
    seq_count = chosen_ref.shape[0]
    blk = tokens_ref.shape[1]
    loads = [
        pltpu.make_async_copy(wq_ref, wq_buf, w_sems.at[0]),
        pltpu.make_async_copy(wk_ref, wk_buf, w_sems.at[1]),
        pltpu.make_async_copy(wv_ref, wv_buf, w_sems.at[2]),
    ]
    small = [
        pltpu.make_async_copy(lengths_in, lengths_ref, w_sems.at[3]),
        pltpu.make_async_copy(chosen_in, chosen_ref, w_sems.at[4]),
    ]
    for load in small + loads[1:]:
        load.start()
    small[0].wait()
    order_by_length(lengths_ref, order_ref, seq_count)
    fetch = [
        pltpu.make_async_copy(
            tokens_ref.at[order_ref[rank]], rows_ref.at[pl.ds(i * blk, blk)], row_sems.at[i]
        )
        for i, rank in enumerate(ranks)
    ]
    for f in fetch[:2] + loads[:1] + fetch[2:]:
        f.start()
    small[1].wait()
    meta_ref[...] = jnp.zeros(meta_ref.shape, jnp.float32)
    for s in range(seq_count):
        meta_ref[s:s + 1, :select] = chosen_ref[s].astype(jnp.float32)
    lane = lax.broadcasted_iota(jnp.int32, meta_ref.shape, 1)
    named = meta_ref[...]
    count = jnp.sum(jnp.where((lane < select) & (named >= 0), 1.0, 0.0), axis=1, keepdims=True)
    meta_ref[...] = jnp.where(lane == select, count, named)
    tile_row = lax.broadcasted_iota(jnp.int32, (META_ROWS, LANES), 0)
    planes = len(ranks) // slots
    for p in range(planes):
        tile = jnp.zeros((META_ROWS, LANES), jnp.float32)
        for j in range(slots):
            row = meta_ref[pl.ds(order_ref[ranks[p * slots + j]], 1), :]
            tile = jnp.where(tile_row == j, row, tile)
        tile = tile.astype(jnp.bfloat16)
        for h in range(kv_local):
            out_ref[p * kv_local + h, slots * 2 * blk:, :] = tile
    stores = []
    for first in range(0, len(ranks), 2):
        fetch[first].wait()
        fetch[first + 1].wait()
        rows = rows_ref[first * blk:(first + 2) * blk, :]
        if first == 0:
            loads[1].wait()
            loads[2].wait()
        k = jnp.dot(rows, wk_buf[...], preferred_element_type=jnp.float32).astype(jnp.bfloat16)
        v = jnp.dot(rows, wv_buf[...], preferred_element_type=jnp.float32).astype(jnp.bfloat16)
        if first == 0:
            loads[0].wait()
        q = jnp.dot(rows, wq_buf[...], preferred_element_type=jnp.float32).astype(jnp.bfloat16)
        for h in range(kv_local):
            q_h = q[:, h * LANES:(h + 1) * LANES]
            kv_h = jnp.concatenate(
                [k[:, h * HEAD_DIM:(h + 1) * HEAD_DIM], v[:, h * HEAD_DIM:(h + 1) * HEAD_DIM]],
                axis=1,
            )
            for i in range(2):
                p, j = divmod(first + i, slots)
                base = j * 2 * blk
                out_ref[p * kv_local + h, base:base + blk, :] = q_h[i * blk:(i + 1) * blk]
                out_ref[p * kv_local + h, base + blk:base + 2 * blk, :] = kv_h[i * blk:(i + 1) * blk]
        if (first + 2) % slots == 0:
            p = first // slots
            at = pl.ds(p * kv_local, kv_local)
            stores.append(
                pltpu.make_async_copy(out_ref.at[at], sent_ref.at[at], sent_sems.at[p])
            )
            stores[-1].start()
    for store in stores:
        store.wait()


def project(tokens, w_query, w_key, w_value, chosen, lengths, ranks, slots, kv_local, vmem):
    seq_count, blk, width = tokens.shape
    dests = len(ranks) // slots * kv_local
    rows = slots * 2 * blk + META_ROWS
    hbm = pl.BlockSpec(memory_space=HBM)
    return pl.pallas_call(
        functools.partial(
            project_kernel, ranks=ranks, slots=slots, kv_local=kv_local, select=chosen.shape[2]
        ),
        in_specs=[hbm] * 6,
        out_specs=pl.BlockSpec(memory_space=pl.ANY),
        out_shape=jax.ShapeDtypeStruct((dests, rows, LANES), jnp.bfloat16),
        scratch_shapes=[
            pltpu.VMEM((dests, rows, LANES), jnp.bfloat16),
            pltpu.SemaphoreType.DMA((len(ranks) // slots,)),
            pltpu.SMEM((seq_count,), jnp.int32),
            pltpu.VMEM(chosen.shape, jnp.int32),
            pltpu.SMEM((seq_count,), jnp.int32),
            pltpu.VMEM((seq_count, LANES), jnp.float32),
            pltpu.VMEM((len(ranks) * blk, width), jnp.bfloat16),
            pltpu.VMEM(w_query.shape, jnp.bfloat16),
            pltpu.VMEM(w_key.shape, jnp.bfloat16),
            pltpu.VMEM(w_value.shape, jnp.bfloat16),
            pltpu.SemaphoreType.DMA((len(ranks),)),
            pltpu.SemaphoreType.DMA((5,)),
        ],
        compiler_params=pltpu.CompilerParams(vmem_limit_bytes=vmem << 10),
        cost_estimate=pl.CostEstimate(
            flops=2 * len(ranks) * blk * width * 2 * kv_local * LANES,
            transcendentals=0,
            bytes_accessed=2 * (len(ranks) * blk * width + w_query.size * 2 + dests * rows * LANES),
        ),
        name="project",
    )(lengths, chosen, tokens, w_query, w_key, w_value)


def attend_kernel(
    lengths_ref, where_ref, list_ref, *refs, early, split, planes, blocks, blk, stride, sizes,
):
    plane, start = where_ref[0], where_ref[1]
    first_half = start == 0
    if early:
        arrived, out_ref, order_ref, o_buf, out_sem = refs
        part = 0
    else:
        own, arrived = refs[0], refs[1]
        far = refs[2:2 + split]
        out_ref, order_ref, o_buf, out_sem = refs[3 + split:]
        part = jnp.where(first_half, 1, 0)

    def near_block(j, b, at):
        rows = pl.ds(pl.multiple_of(j * 2 * blk + at, blk), blk)
        if early:
            return arrived[b, rows, :]
        return jnp.where(first_half, arrived[b, rows, :], own[b, rows, :])

    def key_block(j, c):
        if early:
            return near_block(j, c, blk)
        near = near_block(j, jnp.maximum(c - start, 0), blk)
        at = jnp.minimum(c, blocks - 1)
        other = far[0][at]
        for k in range(1, split):
            other = jnp.where(j == k, far[k][at], other)
        return jnp.where(c >= start, near, other)

    lane = lax.broadcasted_iota(jnp.int32, (blk, LANES), 1)
    low = lane < HEAD_DIM
    row = lax.broadcasted_iota(jnp.int32, (2 * blk, blk), 0) % blk
    col = lax.broadcasted_iota(jnp.int32, (2 * blk, blk), 1)
    scale = HEAD_DIM ** -0.5

    def list_at(j, b):
        kind = 0 if early else part * blocks
        return ((kind + b) * split + j) * LANES

    def head_rows(j, b):
        q = near_block(j, b, 0).astype(jnp.float32)
        q1 = jnp.where(low, pltpu.roll(q, HEAD_DIM, 1), 0.0)
        q0 = jnp.where(low, q, 0.0)
        return (jnp.concatenate([q0, q1], axis=0) * scale).astype(jnp.bfloat16)

    def body(j, b, length, total):
        meta = list_at(j, b)
        count = list_ref[meta + stride]
        q2 = head_rows(j, b)
        kv = jnp.concatenate(
            [key_block(j, jnp.maximum(list_ref[meta + t], 0)) for t in range(total)], axis=0
        )
        s = lax.dot_general(q2, kv, (((1,), (1,)), ((), ())), preferred_element_type=jnp.float32)
        parts = []
        for t in range(total):
            piece = s[:, t * blk:(t + 1) * blk]
            if t == 0:
                piece = jnp.where(col <= row, piece, -1e30)
            else:
                piece = jnp.where(t < count, piece, -1e30)
            parts.append(piece)
        peak = parts[0]
        for piece in parts[1:]:
            peak = jnp.maximum(peak, piece)
        m = jnp.max(peak, axis=1, keepdims=True)
        p = jnp.concatenate([jnp.exp(piece - m).astype(jnp.bfloat16) for piece in parts], axis=1)
        low_rows = lax.broadcasted_iota(jnp.int32, kv.shape, 1) < HEAD_DIM
        values = jnp.where(low_rows, jnp.ones_like(kv), kv)
        o = jnp.dot(p, values, preferred_element_type=jnp.float32)
        turned = pltpu.roll(o, HEAD_DIM, 1)
        o = jnp.where(low, turned[:blk] / o[:blk], o[blk:] / turned[blk:])
        pos = (start + b) * blk + lax.broadcasted_iota(jnp.int32, (blk, LANES), 0)
        o_buf[b, pl.ds(pl.multiple_of(j * blk, blk), blk), :] = jnp.where(
            pos < length, o, 0.0
        ).astype(jnp.bfloat16)

    def run():
        order_by_length(lengths_ref, order_ref, lengths_ref.shape[0])

        @pl.loop(0, split * blocks // 2)
        def _(step):
            j, b = step // (blocks // 2), step % (blocks // 2) * 2
            slot = part * split + j
            rank = slot * planes + jnp.where(slot % 2 == 0, plane, planes - 1 - plane)
            length = lengths_ref[order_ref[rank]]
            need = jnp.maximum(
                list_ref[list_at(j, b) + stride], list_ref[list_at(j, b + 1) + stride]
            )
            live = (start + b) * blk < length
            less = 0
            for size in sizes:
                @pl.when(live & (need > less) & (need <= size))
                def _():
                    body(j, b, length, size)
                    body(j, b + 1, length, size)

                less = size

        at = pl.ds(0 if early else pl.multiple_of(part * split * blk, split * blk), split * blk)
        store = pltpu.make_async_copy(o_buf, out_ref.at[:, at, :], out_sem)
        store.start()
        store.wait()

    if early:
        pl.when(first_half)(run)
    else:
        run()


def attend(lengths, where, lists, operands, early, split, planes, blk, stride):
    blocks = operands[0].shape[0]
    smem = pl.BlockSpec(memory_space=pltpu.SMEM)
    vmem = pl.BlockSpec(memory_space=pltpu.VMEM)
    anywhere = pl.BlockSpec(memory_space=pl.ANY)
    most = blocks if early else 2 * blocks
    sizes = tuple(n for n in (2, 4, 6, 8, 10, 12, 16) if n < most) + (most,)
    return pl.pallas_call(
        functools.partial(
            attend_kernel, early=early, split=split, planes=planes, blocks=blocks, blk=blk,
            stride=stride, sizes=sizes,
        ),
        in_specs=[smem, smem, smem]
        + [vmem] * (len(operands) - (0 if early else 1))
        + ([] if early else [anywhere]),
        out_specs=anywhere,
        out_shape=jax.ShapeDtypeStruct((blocks, 2 * split * blk, LANES), jnp.bfloat16),
        scratch_shapes=[
            pltpu.SMEM(lengths.shape, jnp.int32),
            pltpu.VMEM((blocks, split * blk, LANES), jnp.bfloat16),
            pltpu.SemaphoreType.DMA,
        ],
        input_output_aliases={} if early else {2 + len(operands): 0},
        compiler_params=pltpu.CompilerParams(vmem_limit_bytes=40 << 20),
        cost_estimate=pl.CostEstimate(
            flops=4 * 2 * blk * blk * LANES * blocks * blocks * split,
            transcendentals=0,
            bytes_accessed=3 << 20,
        ),
        name="attend_early" if early else "attend",
    )(lengths, where, lists, *operands)


def output_kernel(
    lengths_ref, side_ref, own_ref, other_ref, w_ref, out_ref,
    order_ref, rows_buf, out_sems, *, planes, kv_local,
):
    seq_count, blk = out_ref.shape[0], out_ref.shape[1]
    order_by_length(lengths_ref, order_ref, seq_count)
    half = kv_local * LANES
    own_at = pl.multiple_of(side_ref[0] * half, half)
    other_at = pl.multiple_of((1 - side_ref[0]) * half, half)

    def rows(ref, rank):
        p, j = place(rank, planes)
        return jnp.concatenate(
            [ref[p * kv_local + h, j * blk:(j + 1) * blk, :] for h in range(kv_local)], axis=1
        )

    stores = []
    for rank in range(0, seq_count, 2):
        mine = jnp.concatenate([rows(own_ref, rank), rows(own_ref, rank + 1)], axis=0)
        theirs = jnp.concatenate([rows(other_ref, rank), rows(other_ref, rank + 1)], axis=0)
        o = jnp.dot(mine, w_ref[pl.ds(own_at, half), :], preferred_element_type=jnp.float32)
        o = o + jnp.dot(
            theirs, w_ref[pl.ds(other_at, half), :], preferred_element_type=jnp.float32
        )
        for r in (rank, rank + 1):
            live = side_ref[1] < lengths_ref[order_ref[r]]
            rows_buf[r] = jnp.where(
                live, o[(r - rank) * blk:(r - rank + 1) * blk], 0.0
            ).astype(jnp.bfloat16)
            store = pltpu.make_async_copy(
                rows_buf.at[r], out_ref.at[order_ref[r]], out_sems.at[r]
            )
            store.start()
            stores.append(store)
    for store in stores:
        store.wait()


def output_projection(own, other, w_output, lengths, side, planes, kv_local, blk):
    seq_count = lengths.shape[0]
    width = w_output.shape[1]
    smem = pl.BlockSpec(memory_space=pltpu.SMEM)
    vmem = pl.BlockSpec(memory_space=pltpu.VMEM)
    hbm = pl.BlockSpec(memory_space=HBM)
    return pl.pallas_call(
        functools.partial(output_kernel, planes=planes, kv_local=kv_local),
        in_specs=[smem, smem, vmem, vmem, vmem],
        out_specs=hbm,
        out_shape=jax.ShapeDtypeStruct((seq_count, blk, width), jnp.bfloat16),
        scratch_shapes=[
            pltpu.SMEM((seq_count,), jnp.int32),
            pltpu.VMEM((seq_count, blk, width), jnp.bfloat16),
            pltpu.SemaphoreType.DMA((seq_count,)),
        ],
        compiler_params=pltpu.CompilerParams(vmem_limit_bytes=40 << 20),
        cost_estimate=pl.CostEstimate(
            flops=2 * seq_count * blk * w_output.size, transcendentals=0, bytes_accessed=6 << 20
        ),
        name="output_projection",
    )(lengths, side, own, other, w_output)


def place(rank, planes):
    j, step = divmod(rank, planes)
    return (step if j % 2 == 0 else planes - 1 - step), j


def per_device(tokens, w_query, w_key, w_value, w_output, chosen, lengths):
    seq_count, blk, _ = tokens.shape
    kv_devices = lax.axis_size("kv")
    kv_local = w_key.shape[1] // HEAD_DIM
    half = kv_devices // 2
    planes = half // kv_local
    slots = seq_count // planes
    split = slots // 2
    select = chosen.shape[2]
    ranks = {place(rank, planes): rank for rank in range(seq_count)}
    groups = [
        tuple(ranks[p, part * split + j] for p in range(planes) for j in range(split))
        for part in range(2)
    ]
    halves = [list(range(half)), list(range(half, kv_devices))]

    def exchange(x):
        return lax.all_to_all(
            x, "kv", split_axis=0, concat_axis=0, tiled=True, axis_index_groups=halves
        )

    def lists_of(arrived):
        at = split * 2 * blk
        return arrived[:, at:at + split, :].astype(jnp.int32)

    def to_second_half(x):
        return lax.ppermute(x, "kv", [(i, i + half) for i in range(half)])

    here = lax.axis_index("kv").astype(jnp.int32)
    where = jnp.stack([here % half // kv_local, here // half * half])
    sent_a = project(tokens, w_query, w_key, w_value, chosen, lengths, groups[0], split, kv_local, 64000)
    arrived_a = exchange(sent_a)
    later, _ = lax.optimization_barrier((lengths, sent_a))
    sent_b = project(tokens, w_query, w_key, w_value, chosen, later, groups[1], split, kv_local, 61440)
    long_count = jnp.sum((lengths > half * blk).astype(jnp.int32))
    sent_b, long_count = lax.optimization_barrier((sent_b, long_count))
    lists_a = lists_of(arrived_a)
    started = attend(
        lengths, where, lists_a.reshape(-1), [arrived_a], True, split, planes, blk, select
    )

    def keys_of(arrived, j):
        return arrived[:, (2 * j + 1) * blk:(2 * j + 2) * blk, :]

    from_half = [to_second_half(keys_of(arrived_a, 0))]
    for j in range(1, split):
        from_half.append(
            lax.cond(
                long_count > j * planes,
                lambda x: to_second_half(keys_of(x, j)),
                lambda x: jnp.zeros((half, blk, LANES), x.dtype),
                arrived_a,
            )
        )
    arrived_b = exchange(sent_b)
    lists = jnp.concatenate([lists_a, lists_of(arrived_b)]).reshape(-1)
    attended = attend(
        lengths, where, lists, [arrived_a, arrived_b] + from_half + [started], False, split,
        planes, blk, select,
    )
    own = exchange(attended)
    other = lax.ppermute(own, "tp", [(0, 1), (1, 0)])
    side = jnp.stack([lax.axis_index("tp").astype(jnp.int32), here * blk])
    return output_projection(own, other, w_output, lengths, side, planes, kv_local, blk)


def fits(mesh, tokens, w_key, chosen):
    seq_count, seq_len = tokens.shape[0], tokens.shape[1]
    kv_devices, tp_devices = mesh.shape["kv"], mesh.shape["tp"]
    kv_local = w_key.shape[1] // tp_devices // HEAD_DIM
    if HEADS // KV_HEADS * HEAD_DIM != LANES or 2 * HEAD_DIM != LANES or tp_devices != 2:
        return False
    if kv_local == 0 or kv_devices % (4 * kv_local) or kv_devices > 16 or chosen.shape[2] >= LANES:
        return False
    planes = kv_devices // 2 // kv_local
    if seq_len // kv_devices != LANES or seq_count % (4 * planes):
        return False
    split = seq_count // planes // 2
    fits_half = (seq_count - 1) * seq_len // 4 // (split * planes) <= seq_len // 2
    return split <= META_ROWS and planes * split % 2 == 0 and fits_half


def fits(mesh, tokens, w_key, chosen):
    seq_count, seq_len = tokens.shape[0], tokens.shape[1]
    kv_devices, tp_devices = mesh.shape["kv"], mesh.shape["tp"]
    kv_local = w_key.shape[1] // tp_devices // HEAD_DIM
    if HEADS // KV_HEADS * HEAD_DIM != LANES or 2 * HEAD_DIM != LANES or tp_devices != 2:
        return False
    if kv_local == 0 or kv_devices % (4 * kv_local) or kv_devices > 16 or chosen.shape[2] >= LANES:
        return False
    planes = kv_devices // kv_local
    if seq_len // kv_devices != LANES or seq_count <= planes or seq_count % 2 or planes % 2:
        return False
    slots, odd = divmod(seq_count - planes, planes // 2)
    fits_half = (seq_count - 1) * seq_len // 4 // planes <= seq_len // 2
    return odd == 0 and slots <= META_ROWS and (planes // 2 * slots) % 2 == 0 and fits_half


def solution(mesh):
    def run(tokens, w_query, w_key, w_value, w_output, chosen, lengths):
        def sharded(body):
            return jax.shard_map(
                body,
                mesh=mesh,
                in_specs=(
                    P(None, "kv", None),
                    P(None, "tp"),
                    P(None, "tp"),
                    P(None, "tp"),
                    P(None, "tp"),
                    P(None, "kv", None),
                    P(),
                ),
                out_specs=P(None, "kv", "tp"),
                check_vma=False,
            )

        arrays = (tokens, w_query, w_key, w_value, w_output, chosen, lengths)
        if not fits(mesh, tokens, w_key, chosen):
            return sharded(per_device_general)(*arrays)

        return sharded(per_device)(*arrays)

    return run
```

```python
import functools

import jax
import jax.numpy as jnp
from jax import lax
from jax.experimental import pallas as pl
from jax.experimental.pallas import tpu as pltpu
from jax.sharding import PartitionSpec as P


HEADS = 16
KV_HEADS = 8
HEAD_DIM = 64
CAP = 4
META_ROWS = 16
LANES = 128
HBM = pltpu.HBM


def per_device_general(tokens, w_query, w_key, w_value, w_output, chosen, lengths):
    seq_count, block_len, model_width = tokens.shape
    flat_rows = tokens.reshape(seq_count * block_len, model_width)
    queries = jnp.dot(flat_rows, w_query, preferred_element_type=jnp.float32).astype(jnp.bfloat16)
    key_proj = jnp.dot(flat_rows, w_key, preferred_element_type=jnp.float32).astype(jnp.bfloat16)
    value_proj = jnp.dot(flat_rows, w_value, preferred_element_type=jnp.float32).astype(
        jnp.bfloat16
    )
    key_width = key_proj.shape[1]
    local_blocks = jnp.concatenate([key_proj, value_proj], axis=1).reshape(
        seq_count, block_len, 2 * key_width
    )
    shard_member = lax.axis_index("kv")
    kv_devices = lax.axis_size("kv")
    picked = chosen[:, 0, :]
    clipped = jnp.maximum(picked, 0)
    seq_index = jnp.arange(seq_count, dtype=jnp.int32)
    owners = jnp.arange(kv_devices, dtype=jnp.int32)
    wanted = (
        jnp.any(picked[:, :, None] == owners[None, None, :], axis=1)
        & (owners != shard_member)[None, :]
    )
    wanted = wanted.T
    ranked = jnp.cumsum(wanted.astype(jnp.int32), axis=1) - 1
    slot_hit = wanted[:, :, None] & (
        ranked[:, :, None] == jnp.arange(CAP, dtype=jnp.int32)[None, None, :]
    )
    request = jnp.sum(slot_hit.astype(jnp.int32) * (seq_index + 1)[None, :, None], axis=1) - 1
    incoming = lax.all_to_all(request, "kv", split_axis=0, concat_axis=0, tiled=True)
    outgoing = local_blocks[jnp.maximum(incoming, 0)]
    arrived = lax.all_to_all(outgoing, "kv", split_axis=0, concat_axis=0, tiled=True)
    key_lookup = jnp.concatenate(
        [local_blocks, arrived.reshape(kv_devices * CAP, block_len, 2 * key_width)], axis=0
    )
    rank_at = jnp.take_along_axis(ranked.T, clipped, axis=1)
    source = jnp.where(
        picked == shard_member, seq_index[:, None], seq_count + clipped * CAP + rank_at
    )
    group_size = HEADS // KV_HEADS
    local_kv_heads = key_width // HEAD_DIM
    query_pos = shard_member * block_len + jnp.arange(block_len, dtype=jnp.int32)
    score_scale = HEAD_DIM ** (-0.5)

    def attend(packed):
        query_rows, source_row, pick_row, length = packed
        fetched = key_lookup[source_row]
        slot_count = pick_row.shape[0]
        key_rows = fetched[:, :, :key_width].reshape(
            slot_count * block_len, local_kv_heads, HEAD_DIM
        )
        value_rows = fetched[:, :, key_width:].reshape(
            slot_count * block_len, local_kv_heads, HEAD_DIM
        )
        grouped = query_rows.reshape(block_len, local_kv_heads, group_size, HEAD_DIM)
        scores = (
            jnp.einsum("qkgd,nkd->kgqn", grouped, key_rows, preferred_element_type=jnp.float32)
            * score_scale
        )
        key_pos = (
            pick_row[:, None] * block_len + jnp.arange(block_len, dtype=jnp.int32)[None, :]
        ).reshape(-1)
        listed = jnp.repeat(pick_row >= 0, block_len)
        allowed = (
            listed[None, :] & (key_pos[None, :] <= query_pos[:, None]) & (key_pos[None, :] < length)
        )
        masked = jnp.where(allowed, scores, -1e30)
        row_max = jnp.max(masked, axis=-1, keepdims=True)
        exponent = jnp.exp(masked - row_max)
        weights = (exponent / jnp.sum(exponent, axis=-1, keepdims=True)).astype(jnp.bfloat16)
        mixed_heads = jnp.einsum(
            "kgqn,nkd->qkgd", weights, value_rows, preferred_element_type=jnp.float32
        )
        live_rows = (query_pos < length)[:, None, None, None]
        return jnp.where(live_rows, mixed_heads, 0.0).astype(jnp.bfloat16).reshape(block_len, -1)

    attended = lax.map(attend, (queries.reshape(seq_count, block_len, -1), source, picked, lengths))
    attended_rows = attended.reshape(seq_count * block_len, -1)
    summed = jnp.dot(
        lax.all_gather(attended_rows, "tp", axis=1, tiled=True),
        w_output,
        preferred_element_type=jnp.float32,
    )
    return summed.astype(jnp.bfloat16).reshape(seq_count, block_len, -1)


def order_by_length(lengths_ref, order_ref, seq_count):
    for s in range(seq_count):
        rank = jnp.int32(0)
        for t in range(seq_count):
            if t < s:
                ahead = lengths_ref[t] >= lengths_ref[s]
            elif t > s:
                ahead = lengths_ref[t] > lengths_ref[s]
            else:
                continue
            rank = rank + jnp.where(ahead, 1, 0)
        order_ref[rank] = s


def project_kernel(
    lengths_in, chosen_in, tokens_ref, wq_ref, wk_ref, wv_ref, sent_ref,
    out_ref, sent_sems, lengths_ref, chosen_ref, order_ref, meta_ref, rows_ref, wq_buf, wk_buf, wv_buf, row_sems, w_sems,
    *, ranks, slots, kv_local, select,
):
    seq_count = chosen_ref.shape[0]
    blk = tokens_ref.shape[1]
    loads = [
        pltpu.make_async_copy(wq_ref, wq_buf, w_sems.at[0]),
        pltpu.make_async_copy(wk_ref, wk_buf, w_sems.at[1]),
        pltpu.make_async_copy(wv_ref, wv_buf, w_sems.at[2]),
    ]
    small = [
        pltpu.make_async_copy(lengths_in, lengths_ref, w_sems.at[3]),
        pltpu.make_async_copy(chosen_in, chosen_ref, w_sems.at[4]),
    ]
    for load in small + loads[1:]:
        load.start()
    small[0].wait()
    order_by_length(lengths_ref, order_ref, seq_count)
    fetch = [
        pltpu.make_async_copy(
            tokens_ref.at[order_ref[rank]], rows_ref.at[pl.ds(i * blk, blk)], row_sems.at[i]
        )
        for i, rank in enumerate(ranks)
    ]
    for f in fetch[:2] + loads[:1] + fetch[2:]:
        f.start()
    small[1].wait()
    meta_ref[...] = jnp.zeros(meta_ref.shape, jnp.float32)
    for s in range(seq_count):
        meta_ref[s:s + 1, :select] = chosen_ref[s].astype(jnp.float32)
    lane = lax.broadcasted_iota(jnp.int32, meta_ref.shape, 1)
    named = meta_ref[...]
    count = jnp.sum(jnp.where((lane < select) & (named >= 0), 1.0, 0.0), axis=1, keepdims=True)
    meta_ref[...] = jnp.where(lane == select, count, named)
    tile_row = lax.broadcasted_iota(jnp.int32, (META_ROWS, LANES), 0)
    planes = len(ranks) // slots
    for p in range(planes):
        tile = jnp.zeros((META_ROWS, LANES), jnp.float32)
        for j in range(slots):
            row = meta_ref[pl.ds(order_ref[ranks[p * slots + j]], 1), :]
            tile = jnp.where(tile_row == j, row, tile)
        tile = tile.astype(jnp.bfloat16)
        for h in range(kv_local):
            out_ref[p * kv_local + h, slots * 2 * blk:, :] = tile
    stores = []
    for first in range(0, len(ranks), 2):
        fetch[first].wait()
        fetch[first + 1].wait()
        rows = rows_ref[first * blk:(first + 2) * blk, :]
        if first == 0:
            loads[1].wait()
            loads[2].wait()
        k = jnp.dot(rows, wk_buf[...], preferred_element_type=jnp.float32).astype(jnp.bfloat16)
        v = jnp.dot(rows, wv_buf[...], preferred_element_type=jnp.float32).astype(jnp.bfloat16)
        if first == 0:
            loads[0].wait()
        q = jnp.dot(rows, wq_buf[...], preferred_element_type=jnp.float32).astype(jnp.bfloat16)
        for h in range(kv_local):
            q_h = q[:, h * LANES:(h + 1) * LANES]
            kv_h = jnp.concatenate(
                [k[:, h * HEAD_DIM:(h + 1) * HEAD_DIM], v[:, h * HEAD_DIM:(h + 1) * HEAD_DIM]],
                axis=1,
            )
            for i in range(2):
                p, j = divmod(first + i, slots)
                base = j * 2 * blk
                out_ref[p * kv_local + h, base:base + blk, :] = q_h[i * blk:(i + 1) * blk]
                out_ref[p * kv_local + h, base + blk:base + 2 * blk, :] = kv_h[i * blk:(i + 1) * blk]
        if (first + 2) % slots == 0:
            p = first // slots
            at = pl.ds(p * kv_local, kv_local)
            stores.append(
                pltpu.make_async_copy(out_ref.at[at], sent_ref.at[at], sent_sems.at[p])
            )
            stores[-1].start()
    for store in stores:
        store.wait()


def project(tokens, w_query, w_key, w_value, chosen, lengths, ranks, slots, kv_local, vmem):
    seq_count, blk, width = tokens.shape
    dests = len(ranks) // slots * kv_local
    rows = slots * 2 * blk + META_ROWS
    hbm = pl.BlockSpec(memory_space=HBM)
    return pl.pallas_call(
        functools.partial(
            project_kernel, ranks=ranks, slots=slots, kv_local=kv_local, select=chosen.shape[2]
        ),
        in_specs=[hbm] * 6,
        out_specs=pl.BlockSpec(memory_space=pl.ANY),
        out_shape=jax.ShapeDtypeStruct((dests, rows, LANES), jnp.bfloat16),
        scratch_shapes=[
            pltpu.VMEM((dests, rows, LANES), jnp.bfloat16),
            pltpu.SemaphoreType.DMA((len(ranks) // slots,)),
            pltpu.SMEM((seq_count,), jnp.int32),
            pltpu.VMEM(chosen.shape, jnp.int32),
            pltpu.SMEM((seq_count,), jnp.int32),
            pltpu.VMEM((seq_count, LANES), jnp.float32),
            pltpu.VMEM((len(ranks) * blk, width), jnp.bfloat16),
            pltpu.VMEM(w_query.shape, jnp.bfloat16),
            pltpu.VMEM(w_key.shape, jnp.bfloat16),
            pltpu.VMEM(w_value.shape, jnp.bfloat16),
            pltpu.SemaphoreType.DMA((len(ranks),)),
            pltpu.SemaphoreType.DMA((5,)),
        ],
        compiler_params=pltpu.CompilerParams(vmem_limit_bytes=vmem << 10),
        cost_estimate=pl.CostEstimate(
            flops=2 * len(ranks) * blk * width * 2 * kv_local * LANES,
            transcendentals=0,
            bytes_accessed=2 * (len(ranks) * blk * width + w_query.size * 2 + dests * rows * LANES),
        ),
        name="project",
    )(lengths, chosen, tokens, w_query, w_key, w_value)


def attend_kernel(
    lengths_ref, where_ref, list_ref, *refs, early, split, planes, blocks, blk, stride, sizes,
):
    plane, start = where_ref[0], where_ref[1]
    first_half = start == 0
    if early:
        arrived, out_ref, order_ref, o_buf, out_sem = refs
        part = 0
    else:
        own, arrived = refs[0], refs[1]
        far = refs[2:2 + split]
        out_ref, order_ref, o_buf, out_sem = refs[3 + split:]
        part = jnp.where(first_half, 1, 0)

    def near_block(j, b, at):
        rows = pl.ds(pl.multiple_of(j * 2 * blk + at, blk), blk)
        if early:
            return arrived[b, rows, :]
        return jnp.where(first_half, arrived[b, rows, :], own[b, rows, :])

    def key_block(j, c):
        if early:
            return near_block(j, c, blk)
        near = near_block(j, jnp.maximum(c - start, 0), blk)
        at = jnp.minimum(c, blocks - 1)
        other = far[0][at]
        for k in range(1, split):
            other = jnp.where(j == k, far[k][at], other)
        return jnp.where(c >= start, near, other)

    lane = lax.broadcasted_iota(jnp.int32, (blk, LANES), 1)
    low = lane < HEAD_DIM
    row = lax.broadcasted_iota(jnp.int32, (2 * blk, blk), 0) % blk
    col = lax.broadcasted_iota(jnp.int32, (2 * blk, blk), 1)
    scale = HEAD_DIM ** -0.5

    def list_at(j, b):
        kind = 0 if early else part * blocks
        return ((kind + b) * split + j) * LANES

    def head_rows(j, b):
        q = near_block(j, b, 0).astype(jnp.float32)
        q1 = jnp.where(low, pltpu.roll(q, HEAD_DIM, 1), 0.0)
        q0 = jnp.where(low, q, 0.0)
        return (jnp.concatenate([q0, q1], axis=0) * scale).astype(jnp.bfloat16)

    def body(j, b, length, total):
        meta = list_at(j, b)
        count = list_ref[meta + stride]
        q2 = head_rows(j, b)
        kv = jnp.concatenate(
            [key_block(j, jnp.maximum(list_ref[meta + t], 0)) for t in range(total)], axis=0
        )
        s = lax.dot_general(q2, kv, (((1,), (1,)), ((), ())), preferred_element_type=jnp.float32)
        parts = []
        for t in range(total):
            piece = s[:, t * blk:(t + 1) * blk]
            if t == 0:
                piece = jnp.where(col <= row, piece, -1e30)
            else:
                piece = jnp.where(t < count, piece, -1e30)
            parts.append(piece)
        peak = parts[0]
        for piece in parts[1:]:
            peak = jnp.maximum(peak, piece)
        m = jnp.max(peak, axis=1, keepdims=True)
        p = jnp.concatenate([jnp.exp(piece - m).astype(jnp.bfloat16) for piece in parts], axis=1)
        low_rows = lax.broadcasted_iota(jnp.int32, kv.shape, 1) < HEAD_DIM
        values = jnp.where(low_rows, jnp.ones_like(kv), kv)
        o = jnp.dot(p, values, preferred_element_type=jnp.float32)
        turned = pltpu.roll(o, HEAD_DIM, 1)
        o = jnp.where(low, turned[:blk] / o[:blk], o[blk:] / turned[blk:])
        pos = (start + b) * blk + lax.broadcasted_iota(jnp.int32, (blk, LANES), 0)
        o_buf[b, pl.ds(pl.multiple_of(j * blk, blk), blk), :] = jnp.where(
            pos < length, o, 0.0
        ).astype(jnp.bfloat16)

    def run():
        order_by_length(lengths_ref, order_ref, lengths_ref.shape[0])

        @pl.loop(0, split * blocks // 2)
        def _(step):
            j, b = step // (blocks // 2), step % (blocks // 2) * 2
            slot = part * split + j
            rank = slot * planes + jnp.where(slot % 2 == 0, plane, planes - 1 - plane)
            length = lengths_ref[order_ref[rank]]
            need = jnp.maximum(
                list_ref[list_at(j, b) + stride], list_ref[list_at(j, b + 1) + stride]
            )
            live = (start + b) * blk < length
            less = 0
            for size in sizes:
                @pl.when(live & (need > less) & (need <= size))
                def _():
                    body(j, b, length, size)
                    body(j, b + 1, length, size)

                less = size

        at = pl.ds(0 if early else pl.multiple_of(part * split * blk, split * blk), split * blk)
        store = pltpu.make_async_copy(o_buf, out_ref.at[:, at, :], out_sem)
        store.start()
        store.wait()

    if early:
        pl.when(first_half)(run)
    else:
        run()


def attend(lengths, where, lists, operands, early, split, planes, blk, stride):
    blocks = operands[0].shape[0]
    smem = pl.BlockSpec(memory_space=pltpu.SMEM)
    vmem = pl.BlockSpec(memory_space=pltpu.VMEM)
    anywhere = pl.BlockSpec(memory_space=pl.ANY)
    most = blocks if early else 2 * blocks
    sizes = tuple(n for n in (2, 4, 6, 8, 10, 12, 16) if n < most) + (most,)
    return pl.pallas_call(
        functools.partial(
            attend_kernel, early=early, split=split, planes=planes, blocks=blocks, blk=blk,
            stride=stride, sizes=sizes,
        ),
        in_specs=[smem, smem, smem]
        + [vmem] * (len(operands) - (0 if early else 1))
        + ([] if early else [anywhere]),
        out_specs=anywhere,
        out_shape=jax.ShapeDtypeStruct((blocks, 2 * split * blk, LANES), jnp.bfloat16),
        scratch_shapes=[
            pltpu.SMEM(lengths.shape, jnp.int32),
            pltpu.VMEM((blocks, split * blk, LANES), jnp.bfloat16),
            pltpu.SemaphoreType.DMA,
        ],
        input_output_aliases={} if early else {2 + len(operands): 0},
        compiler_params=pltpu.CompilerParams(vmem_limit_bytes=40 << 20),
        cost_estimate=pl.CostEstimate(
            flops=4 * 2 * blk * blk * LANES * blocks * blocks * split,
            transcendentals=0,
            bytes_accessed=3 << 20,
        ),
        name="attend_early" if early else "attend",
    )(lengths, where, lists, *operands)


def output_kernel(*refs, planes, kv_local, first):
    if first:
        side_ref, in_ref, w_ref, out_ref, w_next, w_buf, w_sem, next_sem = refs
    else:
        lengths_ref, side_ref, in_ref, w_ref, part_ref, out_ref = refs[:6]
        out_sems, order_ref, rows_buf = refs[6:]
        w_buf = w_ref
    chunks, seq_rows = (out_ref if first else part_ref).shape[:2]
    blk = seq_rows // 2
    half = kv_local * LANES
    if first:
        own_at = pl.multiple_of(side_ref[0] * half, half)
        other_at = pl.multiple_of((1 - side_ref[0]) * half, half)
        load = pltpu.make_async_copy(w_ref.at[pl.ds(own_at, half)], w_buf, w_sem)
        load.start()
        ahead = pltpu.make_async_copy(w_ref.at[pl.ds(other_at, half)], w_next, next_sem)
        ahead.start()
    else:
        order_by_length(lengths_ref, order_ref, 2 * chunks)

    def rows(rank):
        p, j = place(rank, planes)
        return jnp.concatenate(
            [in_ref[p * kv_local + h, j * blk:(j + 1) * blk, :] for h in range(kv_local)], axis=1
        )

    stores = []
    if first:
        load.wait()
        stores.append(ahead)
    for i in range(chunks):
        x = jnp.concatenate([rows(2 * i), rows(2 * i + 1)], axis=0)
        o = jnp.dot(x, w_buf[...], preferred_element_type=jnp.float32)
        if first:
            out_ref[i] = o
            continue
        o = o + part_ref[i]
        for r in (2 * i, 2 * i + 1):
            live = side_ref[1] < lengths_ref[order_ref[r]]
            rows_buf[r] = jnp.where(
                live, o[(r - 2 * i) * blk:(r - 2 * i + 1) * blk], 0.0
            ).astype(jnp.bfloat16)
            stores.append(
                pltpu.make_async_copy(rows_buf.at[r], out_ref.at[order_ref[r]], out_sems.at[r])
            )
            stores[-1].start()
    for store in stores:
        store.wait()


def output_projection(x, part, w_output, lengths, side, planes, kv_local, blk):
    seq_count = lengths.shape[0]
    width = w_output.shape[1]
    first = part is None
    smem = pl.BlockSpec(memory_space=pltpu.SMEM)
    vmem = pl.BlockSpec(memory_space=pltpu.VMEM)
    hbm = pl.BlockSpec(memory_space=HBM)
    sums = (seq_count // 2, 2 * blk, width)
    w_half = (kv_local * LANES, width)
    if first:
        w_output = pltpu.with_memory_space_constraint(w_output, HBM)
        out_shape = [
            jax.ShapeDtypeStruct(sums, jnp.float32), jax.ShapeDtypeStruct(w_half, jnp.bfloat16)
        ]
        specs, operands = [smem, vmem, hbm], (side, x, w_output)
        scratch = [
            pltpu.VMEM(w_half, jnp.bfloat16), pltpu.SemaphoreType.DMA, pltpu.SemaphoreType.DMA
        ]
    else:
        out_shape = jax.ShapeDtypeStruct((seq_count, blk, width), jnp.bfloat16)
        specs, operands = [smem, smem, vmem, vmem, vmem], (lengths, side, x, w_output, part)
        scratch = [
            pltpu.SemaphoreType.DMA((seq_count,)),
            pltpu.SMEM((seq_count,), jnp.int32),
            pltpu.VMEM((seq_count, blk, width), jnp.bfloat16),
        ]
    return pl.pallas_call(
        functools.partial(output_kernel, planes=planes, kv_local=kv_local, first=first),
        in_specs=specs,
        out_specs=[vmem, pl.BlockSpec(memory_space=pl.ANY)] if first else hbm,
        out_shape=out_shape,
        scratch_shapes=scratch,
        compiler_params=pltpu.CompilerParams(vmem_limit_bytes=40 << 20),
        cost_estimate=pl.CostEstimate(
            flops=2 * seq_count * blk * kv_local * LANES * width, transcendentals=0, bytes_accessed=6 << 20
        ),
        name="output_own" if first else "output_other",
    )(*operands)


def place(rank, planes):
    j, step = divmod(rank, planes)
    return (step if j % 2 == 0 else planes - 1 - step), j


def per_device(tokens, w_query, w_key, w_value, w_output, chosen, lengths):
    seq_count, blk, _ = tokens.shape
    kv_devices = lax.axis_size("kv")
    kv_local = w_key.shape[1] // HEAD_DIM
    half = kv_devices // 2
    planes = half // kv_local
    slots = seq_count // planes
    split = slots // 2
    select = chosen.shape[2]
    ranks = {place(rank, planes): rank for rank in range(seq_count)}
    groups = [
        tuple(ranks[p, part * split + j] for p in range(planes) for j in range(split))
        for part in range(2)
    ]
    halves = [list(range(half)), list(range(half, kv_devices))]

    def exchange(x):
        return lax.all_to_all(
            x, "kv", split_axis=0, concat_axis=0, tiled=True, axis_index_groups=halves
        )

    def lists_of(arrived):
        at = split * 2 * blk
        return arrived[:, at:at + split, :].astype(jnp.int32)

    def to_second_half(x):
        return lax.ppermute(x, "kv", [(i, i + half) for i in range(half)])

    here = lax.axis_index("kv").astype(jnp.int32)
    where = jnp.stack([here % half // kv_local, here // half * half])
    sent_a = project(tokens, w_query, w_key, w_value, chosen, lengths, groups[0], split, kv_local, 64000)
    arrived_a = exchange(sent_a)
    later, _ = lax.optimization_barrier((lengths, sent_a))
    sent_b = project(tokens, w_query, w_key, w_value, chosen, later, groups[1], split, kv_local, 61440)
    long_count = jnp.sum((lengths > half * blk).astype(jnp.int32))
    sent_b, long_count = lax.optimization_barrier((sent_b, long_count))
    lists_a = lists_of(arrived_a)
    started = attend(
        lengths, where, lists_a.reshape(-1), [arrived_a], True, split, planes, blk, select
    )

    def keys_of(arrived, j):
        return arrived[:, (2 * j + 1) * blk:(2 * j + 2) * blk, :]

    from_half = [to_second_half(keys_of(arrived_a, 0))]
    for j in range(1, split):
        from_half.append(
            lax.cond(
                long_count > j * planes,
                lambda x: to_second_half(keys_of(x, j)),
                lambda x: jnp.zeros((half, blk, LANES), x.dtype),
                arrived_a,
            )
        )
    arrived_b = exchange(sent_b)
    lists = jnp.concatenate([lists_a, lists_of(arrived_b)]).reshape(-1)
    attended = attend(
        lengths, where, lists, [arrived_a, arrived_b] + from_half + [started], False, split,
        planes, blk, select,
    )
    own = exchange(attended)
    other = lax.ppermute(own, "tp", [(0, 1), (1, 0)])
    side = jnp.stack([lax.axis_index("tp").astype(jnp.int32), here * blk])
    finish = functools.partial(
        output_projection, lengths=lengths, side=side, planes=planes,
        kv_local=kv_local, blk=blk,
    )
    part, w_next = finish(own, None, w_output)
    return finish(other, part, w_next)


def fits(mesh, tokens, w_key, chosen):
    seq_count, seq_len = tokens.shape[0], tokens.shape[1]
    kv_devices, tp_devices = mesh.shape["kv"], mesh.shape["tp"]
    kv_local = w_key.shape[1] // tp_devices // HEAD_DIM
    if HEADS // KV_HEADS * HEAD_DIM != LANES or 2 * HEAD_DIM != LANES or tp_devices != 2:
        return False
    if kv_local == 0 or kv_devices % (4 * kv_local) or kv_devices > 16 or chosen.shape[2] >= LANES:
        return False
    planes = kv_devices // 2 // kv_local
    if seq_len // kv_devices != LANES or seq_count % (4 * planes):
        return False
    split = seq_count // planes // 2
    fits_half = (seq_count - 1) * seq_len // 4 // (split * planes) <= seq_len // 2
    return split <= META_ROWS and planes * split % 2 == 0 and fits_half


def fits(mesh, tokens, w_key, chosen):
    seq_count, seq_len = tokens.shape[0], tokens.shape[1]
    kv_devices, tp_devices = mesh.shape["kv"], mesh.shape["tp"]
    kv_local = w_key.shape[1] // tp_devices // HEAD_DIM
    if HEADS // KV_HEADS * HEAD_DIM != LANES or 2 * HEAD_DIM != LANES or tp_devices != 2:
        return False
    if kv_local == 0 or kv_devices % (4 * kv_local) or kv_devices > 16 or chosen.shape[2] >= LANES:
        return False
    planes = kv_devices // kv_local
    if seq_len // kv_devices != LANES or seq_count <= planes or seq_count % 2 or planes % 2:
        return False
    slots, odd = divmod(seq_count - planes, planes // 2)
    fits_half = (seq_count - 1) * seq_len // 4 // planes <= seq_len // 2
    return odd == 0 and slots <= META_ROWS and (planes // 2 * slots) % 2 == 0 and fits_half


def solution(mesh):
    def run(tokens, w_query, w_key, w_value, w_output, chosen, lengths):
        def sharded(body):
            return jax.shard_map(
                body,
                mesh=mesh,
                in_specs=(
                    P(None, "kv", None),
                    P(None, "tp"),
                    P(None, "tp"),
                    P(None, "tp"),
                    P(None, "tp"),
                    P(None, "kv", None),
                    P(),
                ),
                out_specs=P(None, "kv", "tp"),
                check_vma=False,
            )

        arrays = (tokens, w_query, w_key, w_value, w_output, chosen, lengths)
        if not fits(mesh, tokens, w_key, chosen):
            return sharded(per_device_general)(*arrays)

        return sharded(per_device)(*arrays)

    return run
```
